512 devices in a mesh: sp: 64 (over z, y), tp: 8 (over x, core).
Axes of the slice: x: 4, y: 8, z: 8, core: 2. Of those that a mesh axis runs over, the one named last changes fastest.
Arguments:
- residual: bfloat16 [2048, 16384], P('tp', 'sp'), may hold values from -6 to 6
- values: bfloat16 [16384, 4096], P('sp', 'tp'), may hold values from -6 to 6
- gate_input: bfloat16 [16384, 4096], P('sp', 'tp'), may hold values from -6 to 6
- group_keys: bfloat16 [16384, 3072], P('sp', 'tp'), may hold values from -6 to 6
- time_step: float32 [64, 16384], P('tp', 'sp'), may hold values from -8 to 14
- decay_rate: float32 [64], P('tp'), may hold values from 0 to 2
- skip_gain: float32 [64], P('tp'), may hold values from 0.25 to 2
- conv_values: bfloat16 [4, 4096], P(None, 'tp'), may hold values from -3 to 3
- conv_keys: bfloat16 [4, 3072], P(None, 'tp'), may hold values from -3 to 3
- mix_gain: float32 [4096], P('tp'), may hold values from 0.1 to 1.9
- out_weight: bfloat16 [4096, 2048], P('tp'), may hold values from -0.09375 to 0.09375
- norm_gain: float32 [2048], replicated, may hold values from 0.1 to 1.9
- hidden_gate: bfloat16 [2048, 5120], P('sp', 'tp'), may hold values from -0.125 to 0.125
- hidden_up: bfloat16 [2048, 5120], P('sp', 'tp'), may hold values from -0.125 to 0.125
- hidden_conv: bfloat16 [2, 3, 5120], P(None, None, 'tp'), may hold values from -3.5 to 3.5
- hidden_down: bfloat16 [5120, 2048], P('tp', 'sp'), may hold values from -0.078125 to 0.078125
Outputs:
- layer_out: bfloat16 [2048, 16384], P('tp', 'sp')
The draws below stay inside these ranges and needn't reach their ends.
All inputs are finite; a program needn't handle non-finite values.
Results may differ from the reference program's by a relative error of at most 0.019.
Values may be sent and summed in bfloat16 or wider, within the bound.
No kernel may reach another device: no remote copies, remote signals or barrier semaphores. Data moves between devices by JAX's collectives and lax.ppermute only.
A program may use at most 64 MiB of HBM per device.

```python
import math
import jax
import jax.numpy as jnp
from jax import lax

D = 2048
GROUPS = 8
GROUP_HEADS = 8
HEAD_SIZE = 64
STATE_WIDE = 128
STATE_NARROW = 64
FF = 5120
BLOCK = 128
SHORT_CONV = 4
HIDDEN_CONV = 3
TOK_DEV = 256
TOKENS = 16384
HEADS = 64
INNER = 4096
KEY_COLS = 3072
N_TP = 8


def draw_time_step(key, part):
    key_span = jax.random.fold_in(key, 101)
    key_block = jax.random.fold_in(key, 102)
    key_jitter = jax.random.fold_in(key, 103)
    span_count = TOKENS // TOK_DEV
    span_rank = jnp.arange(span_count, dtype=jnp.float32).reshape(span_count, 1)
    span_trend = 2.5 * (2.0 * span_rank / (span_count - 1) - 1.0)
    span_part = span_trend + jax.random.uniform(key_span, (span_count, 1), jnp.float32, -0.6, 0.6)
    span_part = jnp.broadcast_to(span_part, (span_count, TOK_DEV)).reshape(1, TOKENS)
    block_count = TOKENS // BLOCK
    block_part = jax.random.uniform(key_block, (block_count, 1), jnp.float32, -0.3, 0.3)
    block_part = jnp.broadcast_to(block_part, (block_count, BLOCK)).reshape(1, TOKENS)
    jitter = jnp.clip(0.5 * jax.random.normal(key_jitter, (HEADS, TOKENS), jnp.float32), -1.5, 1.5)
    log_step = math.log(0.1) + span_part + block_part + jitter
    return jnp.log(jnp.expm1(jnp.exp(log_step)))


def draw_decay_rate(key, part):
    key_pick = jax.random.fold_in(key, 201)
    key_fast = jax.random.fold_in(key, 202)
    key_slow = jax.random.fold_in(key, 203)
    fast_share = 0.5
    picked = jax.random.uniform(key_pick, (HEADS,), jnp.float32) < fast_share
    fast_rate = jnp.exp(jax.random.uniform(key_fast, (HEADS,), jnp.float32, math.log(0.1), math.log(0.32)))
    slow_rate = jnp.exp(jax.random.uniform(key_slow, (HEADS,), jnp.float32, math.log(0.3), math.log(4.0))) / TOKENS
    return jnp.where(picked, fast_rate, slow_rate)


def levels(rng, shape, shards, low, largest):
    factor_of, own = 1.0, jax.random.fold_in(rng, 6)
    for position, blocks in shards:
        heights = jnp.exp(jax.random.uniform(jax.random.fold_in(own, position), (blocks,), jnp.float32, low / len(shards), largest / len(shards)))
        factor_of = factor_of * jnp.repeat(heights, shape[position] // blocks).reshape([-1 if axis == position else 1 for axis in range(len(shape))])
    return factor_of


def normal_values(rng, shape, width, reach, split=(), held_as=jnp.bfloat16):
    loudness = levels(rng, shape, split, -0.22, 0.18) if split else 1.0
    drawn = jax.random.normal(rng, shape, jnp.float32) * width * loudness
    return jnp.minimum(jnp.maximum(drawn, -reach), reach).astype(held_as)


def setup_inputs(seed: int = 0) -> dict:
    streams_of = jax.random.split(jax.random.key(seed), 17)
    residual = normal_values(streams_of[0], (D, TOKENS), 1.0, 6.0, ((0, 8), (1, 64)))
    values = normal_values(streams_of[1], (TOKENS, INNER), 1.0, 6.0, ((0, 64), (1, 8)))
    gate_input = normal_values(streams_of[2], (TOKENS, INNER), 1.0, 6.0, ((0, 64), (1, 8)))
    group_keys = normal_values(streams_of[3], (TOKENS, KEY_COLS), 1.0, 6.0, ((0, 64), (1, 8)))
    time_step = draw_time_step(jax.random.fold_in(streams_of[16], 71), 0)
    decay_rate = draw_decay_rate(jax.random.fold_in(streams_of[16], 71), 0)
    skip_gain = jnp.clip(jnp.exp(math.log(2.0) - 2.0794415 * jax.random.uniform(streams_of[6], (HEADS,), jnp.float32) ** levels(streams_of[6], (HEADS,), ((0, 8),), -0.2, 0.2)), 0.25, 2.0)
    conv_values = normal_values(streams_of[7], (SHORT_CONV, INNER), SHORT_CONV ** -0.5, 3.0, ((1, 8),))
    conv_keys = normal_values(streams_of[8], (SHORT_CONV, KEY_COLS), SHORT_CONV ** -0.5, 3.0, ((1, 8),))
    mix_gain = jnp.clip(1.0 + 0.18 * jax.random.normal(streams_of[9], (INNER,), jnp.float32), 0.1, 1.9)
    out_weight = normal_values(streams_of[10], (INNER, D), INNER ** -0.5, 0.09375, ((0, 8),))
    norm_gain = jnp.clip(1.0 + 0.18 * jax.random.normal(streams_of[11], (D,), jnp.float32), 0.1, 1.9)
    hidden_gate = normal_values(streams_of[12], (D, FF), D ** -0.5, 0.125, ((0, 64), (1, 8)))
    hidden_up = normal_values(streams_of[13], (D, FF), D ** -0.5, 0.125, ((0, 64), (1, 8)))
    hidden_conv = normal_values(streams_of[14], (2, HIDDEN_CONV, FF), HIDDEN_CONV ** -0.5, 3.5, ((2, 8),))
    hidden_down = normal_values(streams_of[15], (FF, D), FF ** -0.5, 0.078125, ((0, 8), (1, 64)))
    return dict(residual=residual, values=values, gate_input=gate_input, group_keys=group_keys, time_step=time_step, decay_rate=decay_rate, skip_gain=skip_gain, conv_values=conv_values, conv_keys=conv_keys, mix_gain=mix_gain, out_weight=out_weight, norm_gain=norm_gain, hidden_gate=hidden_gate, hidden_up=hidden_up, hidden_conv=hidden_conv, hidden_down=hidden_down)


NORM_FLOOR = 0.1
HIGHEST = lax.Precision.HIGHEST

def causal_taps(padded, weights, first_row, row_count):
    tap_count = weights.shape[0]
    window = lax.dynamic_slice_in_dim(padded, first_row, row_count + tap_count - 1, 0).astype(jnp.float32)
    summed = weights[0].astype(jnp.float32) * window[0:row_count]
    for tap_index in range(1, tap_count):
        summed = summed + weights[tap_index].astype(jnp.float32) * window[tap_index:tap_index + row_count]
    return summed

def block_heads(inputs, in_keys, out_keys, deltas, decay_rates, skip_table, carried):
    length = inputs.shape[0]
    running = jnp.cumsum(-decay_rates * deltas, axis=0)
    weighted = inputs * deltas[..., None]
    scores = jnp.einsum('ign,jgn->gij', out_keys, in_keys, precision=HIGHEST)
    by_head = jnp.transpose(running, (1, 2, 0))
    between = by_head[..., :, None] - by_head[..., None, :]
    lower_mask = jnp.tril(jnp.ones((length, length), dtype=bool))
    decays = jnp.exp(jnp.where(lower_mask, between, -jnp.inf))
    inside = jnp.einsum('ghij,jghp->ighp', scores[:, None] * decays, weighted, precision=HIGHEST)
    carried_part = jnp.einsum('ign,ghpn->ighp', out_keys, carried, precision=HIGHEST) * jnp.exp(running)[..., None]
    to_end = jnp.exp(by_head[..., -1:] - by_head)
    fresh_state = jnp.einsum('jgn,ghj,jghp->ghpn', in_keys, to_end, weighted, precision=HIGHEST)
    updated = carried * jnp.exp(by_head[..., -1])[..., None, None] + fresh_state
    return (inside + carried_part + inputs * skip_table[..., None], updated)

def sharded_sum(base, left, right, shard_count):
    share = left.shape[1] // shard_count
    summed = base
    for shard in range(shard_count):
        partial_out = jnp.dot(left[:, shard * share:(shard + 1) * share], right[shard * share:(shard + 1) * share], preferred_element_type=jnp.float32)
        partial_out = lax.optimization_barrier(partial_out.astype(jnp.bfloat16))
        summed = summed + partial_out.astype(jnp.float32)
    return summed

def reference(residual, values, gate_input, group_keys, time_step, decay_rate, skip_gain, conv_values, conv_keys, mix_gain, out_weight, norm_gain, hidden_gate, hidden_up, hidden_conv, hidden_down):
    tap_count = conv_values.shape[0]
    pad_values = jnp.pad(values, ((tap_count - 1, 0), (0, 0)))
    pad_keys = jnp.pad(group_keys, ((tap_count - 1, 0), (0, 0)))
    all_deltas = jax.nn.softplus(time_step)
    half_heads = GROUP_HEADS // 2
    wide_end = 2 * STATE_WIDE
    rate_table = decay_rate.reshape(GROUPS, GROUP_HEADS)
    skip_table = skip_gain.reshape(GROUPS, GROUP_HEADS)

    def one_block(carries, block_index):
        first_row = block_index * BLOCK
        inputs = jax.nn.silu(causal_taps(pad_values, conv_values, first_row, BLOCK)).reshape(BLOCK, GROUPS, GROUP_HEADS, HEAD_SIZE)
        key_rows = jax.nn.silu(causal_taps(pad_keys, conv_keys, first_row, BLOCK)).reshape(BLOCK, GROUPS, -1)
        deltas = lax.dynamic_slice_in_dim(all_deltas, first_row, BLOCK, 1).T.reshape(BLOCK, GROUPS, GROUP_HEADS)
        wide_out, wide_state = block_heads(inputs[:, :, :half_heads], key_rows[..., :STATE_WIDE], key_rows[..., STATE_WIDE:wide_end], deltas[:, :, :half_heads], rate_table[:, :half_heads], skip_table[:, :half_heads], carries[0])
        narrow_out, narrow_state = block_heads(inputs[:, :, half_heads:], key_rows[..., wide_end:wide_end + STATE_NARROW], key_rows[..., wide_end + STATE_NARROW:], deltas[:, :, half_heads:], rate_table[:, half_heads:], skip_table[:, half_heads:], carries[1])
        mixer_out = jnp.concatenate([wide_out, narrow_out], axis=2).reshape(BLOCK, INNER)
        gate_rows = lax.dynamic_slice_in_dim(gate_input, first_row, BLOCK, 0).astype(jnp.float32)
        gated_out = mixer_out * jax.nn.silu(gate_rows)
        inverse_rms = lax.rsqrt(lax.optimization_barrier(jnp.mean(gated_out * gated_out, axis=1, keepdims=True)) + NORM_FLOOR)
        normed = (gated_out * inverse_rms * mix_gain).astype(jnp.bfloat16)
        return ((wide_state, narrow_state), normed)
    start_state = (jnp.zeros((GROUPS, half_heads, HEAD_SIZE, STATE_WIDE), jnp.float32), jnp.zeros((GROUPS, GROUP_HEADS - half_heads, HEAD_SIZE, STATE_NARROW), jnp.float32))
    final_state, normed_blocks = lax.scan(one_block, start_state, jnp.arange(TOKENS // BLOCK, dtype=jnp.int32))
    normed_all = normed_blocks.reshape(TOKENS, INNER)
    merged = sharded_sum(residual.T.astype(jnp.float32), normed_all, out_weight, N_TP).astype(jnp.bfloat16)
    merged_wide = merged.astype(jnp.float32)
    inverse_norm = lax.rsqrt(lax.optimization_barrier(jnp.mean(merged_wide * merged_wide, axis=1, keepdims=True)) + NORM_FLOOR)
    lifted = (merged_wide * inverse_norm * norm_gain).astype(jnp.bfloat16)
    gate_pre = jnp.dot(lifted, hidden_gate, preferred_element_type=jnp.float32).astype(jnp.bfloat16)
    up_pre = jnp.dot(lifted, hidden_up, preferred_element_type=jnp.float32).astype(jnp.bfloat16)
    edge_count = hidden_conv.shape[1] - 1
    gate_conv = causal_taps(jnp.pad(gate_pre, ((edge_count, 0), (0, 0))), hidden_conv[0], 0, TOKENS)
    up_conv = causal_taps(jnp.pad(up_pre, ((edge_count, 0), (0, 0))), hidden_conv[1], 0, TOKENS)
    hidden = (jax.nn.silu(gate_conv) * up_conv).astype(jnp.bfloat16)
    layer_out = sharded_sum(merged_wide, hidden, hidden_down, N_TP).astype(jnp.bfloat16)
    return layer_out.T
```

```python
import functools

import jax
import jax.numpy as jnp
from jax import lax
from jax.experimental import pallas as pl
from jax.experimental.pallas import tpu as pltpu
from jax.sharding import Mesh
from jax.sharding import PartitionSpec as P

GROUP_HEADS = 8
HEAD_SIZE = 64
STATE_WIDE = 128
STATE_NARROW = 64
HALF = GROUP_HEADS // 2 * HEAD_SIZE
SP = ("sp_0", "sp_1")
NORM_FLOOR = 0.1
F32 = jnp.float32
BF16 = jnp.bfloat16
HIGHEST = lax.Precision.HIGHEST
LAST = (((1,), (1,)), ((), ()))
FIRST = (((0,), (0,)), ((), ()))


def call(kernel, outs, scratch=(), **more):
    return pl.pallas_call(
        kernel,
        out_shape=[jax.ShapeDtypeStruct(shape, kind) for shape, kind in outs],
        scratch_shapes=[pltpu.VMEM(shape, kind) for shape, kind in scratch],
        **more,
    )


def silu(a):
    return a / (1.0 + jnp.exp(-a))


def pieces(row, count):
    found = []
    for _ in range(count):
        part = row.astype(BF16).astype(F32)
        found.append(part)
        row = row - part
    return found


def head_lanes(cols):
    rows = cols.shape[0]
    lane = lax.broadcasted_iota(jnp.int32, (rows, 2 * HEAD_SIZE), 1)
    both = [
        jnp.where(lane < HEAD_SIZE, cols[:, h : h + 1], cols[:, h + 1 : h + 2])
        for h in range(0, GROUP_HEADS, 2)
    ]
    return jnp.concatenate(both, axis=1)


def as_row(col):
    return jnp.transpose(jnp.broadcast_to(col, (col.shape[0], 128)))[0:1, :]


def as_col(row):
    return jnp.transpose(jnp.broadcast_to(row, (8, row.shape[1])))[:, 0:1]


def conv_silu(buf, taps, rows):
    count = taps.shape[0]
    total = taps[count - 1 : count, :].astype(F32) * buf[8 : 8 + rows, :]
    for k in range(count - 1):
        at = 8 - (count - 1) + k
        total = total + taps[k : k + 1, :].astype(F32) * buf[at : at + rows, :]
    return silu(total)


def state_kernel(
    values, keys, before, step, rate, taps_v, taps_k, x_out, key_out, run_out, delta_out, run_col, pay, vbuf, kbuf
):
    rows, cols = values.shape
    vbuf[0:8, :] = before[:, :cols].astype(F32)
    vbuf[8 : 8 + rows, :] = values[...].astype(F32)
    kbuf[0:8, :] = before[:, cols:].astype(F32)
    kbuf[8 : 8 + rows, :] = keys[...].astype(F32)
    x = conv_silu(vbuf, taps_v, rows)
    k = conv_silu(kbuf, taps_k, rows).astype(BF16)
    x_out[...] = x.astype(BF16)
    key_out[...] = k
    pre = step[...]
    delta = jnp.maximum(pre, 0.0) + jnp.log1p(jnp.exp(-jnp.abs(pre)))
    upper = lax.broadcasted_iota(jnp.int32, (rows, rows), 0) <= lax.broadcasted_iota(
        jnp.int32, (rows, rows), 1
    )
    run = jnp.dot(-rate[...] * delta, upper.astype(F32), precision=HIGHEST, preferred_element_type=F32)
    run_out[...] = run
    delta_out[...] = delta
    run_t = jnp.transpose(run)
    run_col[...] = run_t
    end = run_t[rows - 1 : rows, :]
    to_end = jnp.exp(end - run_t) * jnp.transpose(delta)
    weighted = (x * head_lanes(to_end)).astype(BF16)
    wide = lax.dot_general(k[:, :STATE_WIDE], weighted[:, :HALF], FIRST, preferred_element_type=F32)
    narrow = lax.dot_general(
        k[:, 2 * STATE_WIDE :], weighted[:, HALF:], FIRST, preferred_element_type=F32
    )
    ends = head_lanes(jnp.broadcast_to(end, (8, GROUP_HEADS)))[0:1, :]
    marks = pieces(ends[:, :HALF], 3) + pieces(ends[:, HALF:], 3) + [jnp.zeros((2, HALF), F32)]
    count = pay.shape[0]
    w, n = STATE_WIDE // count, STATE_NARROW // count
    for c in range(count):
        part = [wide[c * w : (c + 1) * w], narrow[c * n : (c + 1) * n]] + marks
        pay[c] = jnp.concatenate(part, axis=0).astype(BF16)


def inside_kernel(x, keys, run, delta, run_col, skip, gate, base_out, slope_out):
    rows = x.shape[0]
    xs = x[...]
    k = keys[...]
    wide_end = 2 * STATE_WIDE
    score_w = lax.dot_general(k[:, STATE_WIDE:wide_end], k[:, :STATE_WIDE], LAST, preferred_element_type=F32)
    score_n = lax.dot_general(
        k[:, wide_end + STATE_NARROW :], k[:, wide_end : wide_end + STATE_NARROW], LAST, preferred_element_type=F32
    )
    keep = lax.broadcasted_iota(jnp.int32, (rows, rows), 0) >= lax.broadcasted_iota(
        jnp.int32, (rows, rows), 1
    )
    runs, deltas, cols = run[...], delta[...], run_col[...]
    outs = []
    for h in range(GROUP_HEADS):
        gap = jnp.where(keep, cols[:, h : h + 1] - runs[h : h + 1, :], -jnp.inf)
        score = score_w if h < GROUP_HEADS // 2 else score_n
        mixed = (score * (jnp.exp(gap) * deltas[h : h + 1, :])).astype(BF16)
        outs.append(
            jnp.dot(mixed, xs[:, h * HEAD_SIZE : (h + 1) * HEAD_SIZE], preferred_element_type=F32)
        )
    opened = silu(gate[...].astype(F32))
    direct = jnp.concatenate(outs, axis=1) + skip[...] * xs.astype(F32)
    base_out[...] = direct * opened
    slope_out[...] = head_lanes(jnp.exp(cols)) * opened


def span_parts(piece):
    w = STATE_WIDE // 8
    n = STATE_NARROW // 8
    state = piece[: w + n]
    at = w + n
    wide = piece[at : at + 1] + piece[at + 1 : at + 2] + piece[at + 2 : at + 3]
    narrow = piece[at + 3 : at + 4] + piece[at + 4 : at + 5] + piece[at + 5 : at + 6]
    return state, wide, narrow


def fade(wide, narrow):
    w = STATE_WIDE // 8
    n = STATE_NARROW // 8
    lanes = wide.shape[1]
    return jnp.concatenate(
        [
            jnp.broadcast_to(jnp.exp(wide), (w, lanes)),
            jnp.broadcast_to(jnp.exp(narrow), (n, lanes)),
        ],
        axis=0,
    )


def row_total_kernel(got, pay):
    count = got.shape[0]
    total = None
    for c in range(count):
        state, wide, narrow = span_parts(got[c].astype(F32))
        if total is None:
            total, log_w, log_n = state, wide, narrow
        else:
            total = total * fade(wide, narrow) + state
            log_w, log_n = log_w + wide, log_n + narrow
    marks = pieces(log_w, 3) + pieces(log_n, 3) + [jnp.zeros((2, log_w.shape[1]), F32)]
    piece = jnp.concatenate([total] + marks, axis=0).astype(BF16)
    for c in range(count):
        pay[c] = piece


def prefix_kernel(place, got, totals, pay):
    count = got.shape[0]
    mine = place[0]
    total = jnp.zeros((pay.shape[1] - 8, pay.shape[2]), F32)
    for c in range(totals.shape[0]):
        state, wide, narrow = span_parts(totals[c].astype(F32))
        total = jnp.where(c < mine, total * fade(wide, narrow) + state, total)
    pad = jnp.zeros((8, pay.shape[2]), F32)
    for c in range(count):
        pay[c] = jnp.concatenate([total, pad], axis=0).astype(BF16)
        state, wide, narrow = span_parts(got[c].astype(F32))
        total = total * fade(wide, narrow) + state


def apply_kernel(base, slope, keys, got, gain, weight, pay):
    count = got.shape[0]
    w = STATE_WIDE // count
    n = STATE_NARROW // count
    carried = [got[c].astype(F32) for c in range(count)]
    wide = jnp.concatenate([c[:w] for c in carried], axis=0).astype(BF16)
    narrow = jnp.concatenate([c[w : w + n] for c in carried], axis=0).astype(BF16)
    k = keys[...]
    wide_end = 2 * STATE_WIDE
    from_wide = jnp.dot(k[:, STATE_WIDE:wide_end], wide, preferred_element_type=F32)
    from_narrow = jnp.dot(k[:, wide_end + STATE_NARROW :], narrow, preferred_element_type=F32)
    gated = base[...] + slope[...] * jnp.concatenate([from_wide, from_narrow], axis=1)
    squares = as_row(jnp.sum(gated * gated, axis=1, keepdims=True))
    marks = pieces(squares, 2) + [jnp.zeros((14, squares.shape[1]), F32)]
    marks = jnp.concatenate(marks, axis=0).astype(BF16)
    scaled = (gated * gain[...]).astype(BF16)
    rows, share = scaled.shape[0], pay.shape[2]
    for c in range(pay.shape[0]):
        part = jnp.dot(scaled, weight[:, c * share : (c + 1) * share], preferred_element_type=F32)
        pay[c, 0:rows, :] = part.astype(BF16)
        pay[c, rows : rows + 16, :] = marks


def merge_kernel(channels, got, residual, gain, lifted_out, tile_out, merged_out):
    rows = residual.shape[1]
    total = got[0].astype(F32)
    for c in range(1, got.shape[0]):
        total = total + got[c].astype(F32)
    squares = total[rows : rows + 1] + total[rows + 1 : rows + 2]
    inverse = as_col(lax.rsqrt(squares / channels + NORM_FLOOR))
    merged = jnp.transpose(residual[...].astype(F32)) + inverse * total[:rows]
    merged = merged.astype(BF16).astype(F32)
    merged_out[...] = jnp.transpose(merged).astype(BF16)
    own = as_row(jnp.sum(merged * merged, axis=1, keepdims=True))
    lifted = (merged * gain[...]).astype(BF16)
    lifted_out[...] = lifted
    edge = lifted[rows - 8 :, :].astype(F32)
    tile = pieces(own, 2) + [jnp.zeros((4, own.shape[1]), F32), edge[6:8]]
    tile_out[...] = jnp.concatenate(tile, axis=0).astype(BF16)


def channel_kernel(blocks, features, got, weight_in, weight_out, taps, pay, total, marks, buf, hidden):
    step = pl.program_id(0)
    rows = hidden.shape[0]
    units = hidden.shape[1]

    @pl.when(step < blocks)
    def _():
        mine = got[0]
        part = jnp.dot(mine, weight_in[...], preferred_element_type=F32)
        mark = mine[rows : rows + 16].astype(F32)

        @pl.when(step == 0)
        def _():
            total[...] = part
            marks[...] = mark

        @pl.when(step > 0)
        def _():
            total[...] += part
            marks[...] += mark

    @pl.when(step == blocks - 1)
    def _():
        def inverse_of(at):
            squares = marks[at : at + 1, :] + marks[at + 1 : at + 2, :]
            return as_col(lax.rsqrt(squares / features + NORM_FLOOR))

        own, before = inverse_of(0), inverse_of(8)
        buf[0:8, :] = (total[rows + 8 : rows + 16, :] * before[rows - 8 :, :]).astype(BF16).astype(F32)
        buf[8 : 8 + rows, :] = (total[0:rows, :] * own).astype(BF16).astype(F32)

        def conv(branch):
            first, last = branch * units, (branch + 1) * units
            count = taps.shape[1]
            summed = None
            for k in range(count):
                at = 8 - (count - 1) + k
                term = taps[branch, k : k + 1, :].astype(F32) * buf[at : at + rows, first:last]
                summed = term if summed is None else summed + term
            return summed

        hidden[...] = (silu(conv(0)) * conv(1)).astype(BF16)

    @pl.when(step >= blocks)
    def _():
        pay[0] = lax.dot_general(
            weight_out[...], hidden[...], LAST, preferred_element_type=F32
        ).astype(BF16)


def exchange(parts, axis):
    return lax.all_to_all(parts, axis, split_axis=0, concat_axis=0, tiled=True)


def from_behind(value, axis):
    count = lax.axis_size(axis)
    return lax.ppermute(value, axis, [(source, source + 1) for source in range(count - 1)])


def local(
    residual,
    values,
    gate_input,
    group_keys,
    time_step,
    decay_rate,
    skip_gain,
    conv_values,
    conv_keys,
    mix_gain,
    out_weight,
    norm_gain,
    hidden_gate,
    hidden_up,
    hidden_conv,
    hidden_down,
):
    own_rows = jnp.concatenate([hidden_gate, hidden_up, hidden_down.T], axis=1)
    weights = lax.all_gather(own_rows, SP, axis=0, tiled=True)
    rows, cols = values.shape
    n_tp = lax.axis_size("tp")
    n_row = lax.axis_size(SP[1])
    features = residual.shape[0]
    units = hidden_gate.shape[1]
    tail = jnp.concatenate([values[rows - 8 :], group_keys[rows - 8 :]], axis=1)
    before = from_behind(tail, SP)
    key_cols = group_keys.shape[1]
    span = STATE_WIDE // n_row + STATE_NARROW // n_row + 8
    x, keys, run, delta, run_col, pay = call(
        state_kernel,
        [
            ((rows, cols), BF16),
            ((rows, key_cols), BF16),
            ((GROUP_HEADS, rows), F32),
            ((GROUP_HEADS, rows), F32),
            ((rows, GROUP_HEADS), F32),
            ((n_row, span, HALF), BF16),
        ],
        [((rows + 8, cols), F32), ((rows + 8, key_cols), F32)],
        name="span_state",
    )(
        values,
        group_keys,
        before,
        time_step,
        decay_rate.reshape(-1, 1),
        conv_values,
        conv_keys,
    )
    by_row = exchange(pay, SP[1])
    base, slope = call(
        inside_kernel, [((rows, cols), F32), ((rows, cols), F32)], name="inside_span"
    )(x, keys, run, delta, run_col, jnp.repeat(skip_gain, HEAD_SIZE).reshape(1, -1), gate_input)
    (sums,) = call(
        row_total_kernel, [((lax.axis_size(SP[0]), span, HALF), BF16)], name="row_total"
    )(by_row)
    totals = exchange(sums, SP[0])
    place = lax.axis_index(SP[0]).astype(jnp.int32).reshape(1)
    (starts,) = call(
        prefix_kernel,
        [((n_row, span, HALF), BF16)],
        in_specs=[
            pl.BlockSpec(memory_space=pltpu.SMEM),
            pl.BlockSpec(memory_space=pltpu.VMEM),
            pl.BlockSpec(memory_space=pltpu.VMEM),
        ],
        name="prefix",
    )(place, by_row, totals)
    carried = exchange(starts, SP[1])
    (partial,) = call(
        apply_kernel, [((n_tp, rows + 16, features), BF16)], name="apply_project"
    )(base, slope, keys, carried, mix_gain.reshape(1, -1), out_weight)
    summed = exchange(partial, "tp")
    own_gain = lax.dynamic_slice_in_dim(norm_gain, lax.axis_index("tp") * features, features, 0)
    lifted, tile, merged = call(
        functools.partial(merge_kernel, cols * n_tp),
        [((rows, features), BF16), ((8, features), BF16), ((features, rows), BF16)],
        name="merge",
    )(summed, residual, own_gain.reshape(1, -1))
    stream = jnp.concatenate([lifted, tile, from_behind(tile, SP)], axis=0)
    stream = exchange(jnp.broadcast_to(stream, (n_tp, *stream.shape)), "tp")
    down_first = 2 * units // units
    (down,) = call(
        functools.partial(channel_kernel, n_tp, features * n_tp),
        [((n_tp, features, rows), BF16)],
        [
            ((rows + 16, 2 * units), F32),
            ((16, features), F32),
            ((rows + 8, 2 * units), F32),
            ((rows, units), BF16),
        ],
        grid=(2 * n_tp,),
        in_specs=[
            pl.BlockSpec((1, rows + 16, features), lambda i: (jnp.minimum(i, n_tp - 1), 0, 0)),
            pl.BlockSpec((features, 2 * units), lambda i: (jnp.minimum(i, n_tp - 1), 0)),
            pl.BlockSpec((features, units), lambda i: (jnp.maximum(i - n_tp, 0), down_first)),
            pl.BlockSpec(hidden_conv.shape, lambda i: (0, 0, 0)),
        ],
        out_specs=[pl.BlockSpec((1, features, rows), lambda i: (jnp.maximum(i - n_tp, 0), 0, 0))],
        name="channel_mixer",
    )(stream, weights, weights, hidden_conv)
    got = exchange(down, "tp")
    return (merged.astype(F32) + jnp.sum(got.astype(F32), axis=0)).astype(BF16)


def solution(mesh):
    split = Mesh(mesh.devices.reshape(8, 8, mesh.shape["tp"]), ("sp_0", "sp_1", "tp"))
    placed = (
        P("tp", SP),
        P(SP, "tp"),
        P(SP, "tp"),
        P(SP, "tp"),
        P("tp", SP),
        P("tp"),
        P("tp"),
        P(None, "tp"),
        P(None, "tp"),
        P("tp"),
        P("tp", None),
        P(),
        P(SP, "tp"),
        P(SP, "tp"),
        P(None, None, "tp"),
        P("tp", SP),
    )
    return jax.shard_map(local, mesh=split, in_specs=placed, out_specs=P("tp", SP), check_vma=False)
```

```python
import functools

import jax
import jax.numpy as jnp
from jax import lax
from jax.experimental import pallas as pl
from jax.experimental.pallas import tpu as pltpu
from jax.sharding import Mesh
from jax.sharding import PartitionSpec as P

GROUP_HEADS = 8
HEAD_SIZE = 64
STATE_WIDE = 128
STATE_NARROW = 64
HALF = GROUP_HEADS // 2 * HEAD_SIZE
SP = ("sp_0", "sp_1")
NORM_FLOOR = 0.1
F32 = jnp.float32
BF16 = jnp.bfloat16
HIGHEST = lax.Precision.HIGHEST
LAST = (((1,), (1,)), ((), ()))
FIRST = (((0,), (0,)), ((), ()))


SMEM = pl.BlockSpec(memory_space=pltpu.SMEM)
VMEM = pl.BlockSpec(memory_space=pltpu.VMEM)


def call(kernel, outs, scratch=(), grant=12, more_scratch=(), **more):
    return pl.pallas_call(
        kernel,
        out_shape=[jax.ShapeDtypeStruct(shape, kind) for shape, kind in outs],
        scratch_shapes=[pltpu.VMEM(shape, kind) for shape, kind in scratch] + list(more_scratch),
        compiler_params=pltpu.CompilerParams(vmem_limit_bytes=grant << 20),
        **more,
    )


def pack_kernel(gate, up, down, values, keys, rows_out, tail_out):
    units = gate.shape[1]
    cols = values.shape[1]
    rows_out[:, :units] = gate[...]
    rows_out[:, units : 2 * units] = up[...]
    rows_out[:, 2 * units :] = down[...]
    tail_out[:, :cols] = values[...]
    tail_out[:, cols:] = keys[...]


def silu(a):
    return a / (1.0 + jnp.exp(-a))


def pieces(row, count):
    found = []
    for _ in range(count):
        part = row.astype(BF16).astype(F32)
        found.append(part)
        row = row - part
    return found


def head_lanes(cols):
    rows = cols.shape[0]
    lane = lax.broadcasted_iota(jnp.int32, (rows, 2 * HEAD_SIZE), 1)
    both = [
        jnp.where(lane < HEAD_SIZE, cols[:, h : h + 1], cols[:, h + 1 : h + 2])
        for h in range(0, GROUP_HEADS, 2)
    ]
    return jnp.concatenate(both, axis=1)


def as_row(col):
    return jnp.transpose(jnp.broadcast_to(col, (col.shape[0], 128)))[0:1, :]


def as_col(row):
    return jnp.transpose(jnp.broadcast_to(row, (8, row.shape[1])))[:, 0:1]


def conv_silu(buf, taps, rows):
    count = taps.shape[0]
    total = taps[count - 1 : count, :].astype(F32) * buf[8 : 8 + rows, :]
    for k in range(count - 1):
        at = 8 - (count - 1) + k
        total = total + taps[k : k + 1, :].astype(F32) * buf[at : at + rows, :]
    return silu(total)


def state_kernel(
    values, keys, before, step, rate, taps_v, taps_k, x_out, key_out, run_out, delta_out, run_col, pay, vbuf, kbuf
):
    rows, cols = values.shape
    vbuf[0:8, :] = before[:, :cols].astype(F32)
    vbuf[8 : 8 + rows, :] = values[...].astype(F32)
    kbuf[0:8, :] = before[:, cols:].astype(F32)
    kbuf[8 : 8 + rows, :] = keys[...].astype(F32)
    x = conv_silu(vbuf, taps_v, rows)
    k = conv_silu(kbuf, taps_k, rows).astype(BF16)
    x_out[...] = x.astype(BF16)
    key_out[...] = k
    pre = step[...]
    delta = jnp.maximum(pre, 0.0) + jnp.log1p(jnp.exp(-jnp.abs(pre)))
    upper = lax.broadcasted_iota(jnp.int32, (rows, rows), 0) <= lax.broadcasted_iota(
        jnp.int32, (rows, rows), 1
    )
    head = lax.broadcasted_iota(jnp.int32, delta.shape, 0)
    rates = jnp.zeros(delta.shape, F32)
    for h in range(GROUP_HEADS):
        rates = jnp.where(head == h, rate[h], rates)
    run = jnp.dot(-rates * delta, upper.astype(F32), precision=HIGHEST, preferred_element_type=F32)
    run_out[...] = run
    delta_out[...] = delta
    run_t = jnp.transpose(run)
    run_col[...] = run_t
    end = run_t[rows - 1 : rows, :]
    to_end = jnp.exp(end - run_t) * jnp.transpose(delta)
    weighted = (x * head_lanes(to_end)).astype(BF16)
    wide = lax.dot_general(k[:, :STATE_WIDE], weighted[:, :HALF], FIRST, preferred_element_type=F32)
    narrow = lax.dot_general(
        k[:, 2 * STATE_WIDE :], weighted[:, HALF:], FIRST, preferred_element_type=F32
    )
    ends = head_lanes(jnp.broadcast_to(end, (8, GROUP_HEADS)))[0:1, :]
    marks = pieces(ends[:, :HALF], 3) + pieces(ends[:, HALF:], 3) + [jnp.zeros((2, HALF), F32)]
    count = pay.shape[0]
    w, n = STATE_WIDE // count, STATE_NARROW // count
    for c in range(count):
        part = [wide[c * w : (c + 1) * w], narrow[c * n : (c + 1) * n]] + marks
        pay[c] = jnp.concatenate(part, axis=0).astype(BF16)


def inside_kernel(x, keys, run, delta, run_col, skip, gate, base_out, slope_out):
    rows = x.shape[0]
    xs = x[...]
    k = keys[...]
    wide_end = 2 * STATE_WIDE
    score_w = lax.dot_general(k[:, STATE_WIDE:wide_end], k[:, :STATE_WIDE], LAST, preferred_element_type=F32)
    score_n = lax.dot_general(
        k[:, wide_end + STATE_NARROW :], k[:, wide_end : wide_end + STATE_NARROW], LAST, preferred_element_type=F32
    )
    keep = lax.broadcasted_iota(jnp.int32, (rows, rows), 0) >= lax.broadcasted_iota(
        jnp.int32, (rows, rows), 1
    )
    runs, deltas, cols = run[...], delta[...], run_col[...]
    outs = []
    for h in range(GROUP_HEADS):
        gap = jnp.where(keep, cols[:, h : h + 1] - runs[h : h + 1, :], -jnp.inf)
        score = score_w if h < GROUP_HEADS // 2 else score_n
        mixed = (score * (jnp.exp(gap) * deltas[h : h + 1, :])).astype(BF16)
        outs.append(
            jnp.dot(mixed, xs[:, h * HEAD_SIZE : (h + 1) * HEAD_SIZE], preferred_element_type=F32)
        )
    opened = silu(gate[...].astype(F32))
    direct = jnp.concatenate(outs, axis=1) + skip[...] * xs.astype(F32)
    base_out[...] = direct * opened
    slope_out[...] = head_lanes(jnp.exp(cols)) * opened


def span_parts(piece):
    w = STATE_WIDE // 8
    n = STATE_NARROW // 8
    state = piece[: w + n]
    at = w + n
    wide = piece[at : at + 1] + piece[at + 1 : at + 2] + piece[at + 2 : at + 3]
    narrow = piece[at + 3 : at + 4] + piece[at + 4 : at + 5] + piece[at + 5 : at + 6]
    return state, wide, narrow


def fade(wide, narrow):
    w = STATE_WIDE // 8
    n = STATE_NARROW // 8
    lanes = wide.shape[1]
    return jnp.concatenate(
        [
            jnp.broadcast_to(jnp.exp(wide), (w, lanes)),
            jnp.broadcast_to(jnp.exp(narrow), (n, lanes)),
        ],
        axis=0,
    )


def row_total_kernel(got, pay):
    count = got.shape[0]
    total = None
    for c in range(count):
        state, wide, narrow = span_parts(got[c].astype(F32))
        if total is None:
            total, log_w, log_n = state, wide, narrow
        else:
            total = total * fade(wide, narrow) + state
            log_w, log_n = log_w + wide, log_n + narrow
    marks = pieces(log_w, 3) + pieces(log_n, 3) + [jnp.zeros((2, log_w.shape[1]), F32)]
    piece = jnp.concatenate([total] + marks, axis=0).astype(BF16)
    for c in range(count):
        pay[c] = piece


def prefix_kernel(place, got, totals, pay):
    count = got.shape[0]
    mine = place[0]
    total = jnp.zeros((pay.shape[1] - 8, pay.shape[2]), F32)
    for c in range(totals.shape[0]):
        state, wide, narrow = span_parts(totals[c].astype(F32))
        total = jnp.where(c < mine, total * fade(wide, narrow) + state, total)
    pad = jnp.zeros((8, pay.shape[2]), F32)
    for c in range(count):
        pay[c] = jnp.concatenate([total, pad], axis=0).astype(BF16)
        state, wide, narrow = span_parts(got[c].astype(F32))
        total = total * fade(wide, narrow) + state


def apply_kernel(core, base, slope, keys, got, gain, weight, keep, give):
    count = got.shape[0]
    w = STATE_WIDE // count
    n = STATE_NARROW // count
    carried = [got[c].astype(F32) for c in range(count)]
    wide = jnp.concatenate([c[:w] for c in carried], axis=0).astype(BF16)
    narrow = jnp.concatenate([c[w : w + n] for c in carried], axis=0).astype(BF16)
    k = keys[...]
    wide_end = 2 * STATE_WIDE
    from_wide = jnp.dot(k[:, STATE_WIDE:wide_end], wide, preferred_element_type=F32)
    from_narrow = jnp.dot(k[:, wide_end + STATE_NARROW :], narrow, preferred_element_type=F32)
    gated = base[...] + slope[...] * jnp.concatenate([from_wide, from_narrow], axis=1)
    squares = as_row(jnp.sum(gated * gated, axis=1, keepdims=True))
    lanes = squares.shape[1]
    hi_lo = pieces(squares, 2)
    blank = jnp.zeros((2, lanes), F32)
    rest = jnp.zeros((12, lanes), F32)
    marks = jnp.concatenate(hi_lo + [blank, rest], axis=0).astype(BF16)
    given = jnp.concatenate([blank] + hi_lo + [rest], axis=0).astype(BF16)
    scaled = (gated * gain[...]).astype(BF16)
    rows, share = scaled.shape[0], keep.shape[2]
    mine = core[0]
    for target, side, mark in ((give, 1 - mine, given), (keep, mine, marks)):
        for c in range(target.shape[0]):
            at = pl.multiple_of((2 * c + side) * share, share)
            part = jnp.dot(scaled, weight[:, pl.ds(at, share)], preferred_element_type=F32)
            target[c, 0:rows, :] = part.astype(BF16)
            target[c, rows : rows + 16, :] = mark


def merge_kernel(channels, got, residual, gain, lifted_out, tile_out, merged_out):
    rows = residual.shape[1]
    total = got[0].astype(F32)
    for c in range(1, got.shape[0]):
        total = total + got[c].astype(F32)
    squares = jnp.sum(total[rows : rows + 8], axis=0, keepdims=True)
    inverse = as_col(lax.rsqrt(squares / channels + NORM_FLOOR))
    merged = jnp.transpose(residual[...].astype(F32)) + inverse * total[:rows]
    merged = merged.astype(BF16).astype(F32)
    merged_out[...] = jnp.transpose(merged).astype(BF16)
    own = as_row(jnp.sum(merged * merged, axis=1, keepdims=True))
    lifted = (merged * gain[...]).astype(BF16)
    lifted_out[...] = lifted
    edge = lifted[rows - 8 :, :].astype(F32)
    tile = pieces(own, 2) + [jnp.zeros((4, own.shape[1]), F32), edge[6:8]]
    tile_out[...] = jnp.concatenate(tile, axis=0).astype(BF16)


def channel_kernel(features, core, own, other, weights, taps, keep, give, lhs, wide, down, buf, hidden, sems):
    chips, high, share = own.shape
    rows = high - 16
    units = hidden.shape[1]
    step = wide.shape[2]
    copies = []
    for n in range(wide.shape[0]):
        copies.append(
            pltpu.make_async_copy(weights.at[:, n * step : (n + 1) * step], wide.at[n], sems.at[n])
        )
    copies.append(
        pltpu.make_async_copy(weights.at[:, 2 * units :], down, sems.at[wide.shape[0]])
    )
    for copy in copies:
        copy.start()
    mine = core[0]
    marks = jnp.zeros((16, share), F32)
    for c in range(chips):
        first, second = own[c], other[c]
        marks = marks + first[rows:].astype(F32) + second[rows:].astype(F32)
        at = 2 * c * share
        lhs[:, at : at + share] = jnp.where(mine == 0, first, second)
        lhs[:, at + share : at + 2 * share] = jnp.where(mine == 0, second, first)

    def inverse_of(at):
        squares = marks[at : at + 1, :] + marks[at + 1 : at + 2, :]
        return as_col(lax.rsqrt(squares / features + NORM_FLOOR))

    scale, before = inverse_of(0), inverse_of(8)
    for n in range(wide.shape[0]):
        copies[n].wait()
        total = jnp.dot(lhs[...], wide[n], preferred_element_type=F32)
        at = n * step
        edge = total[rows + 8 :] * before[rows - 8 :, :]
        buf[0:8, at : at + step] = edge.astype(BF16).astype(F32)
        buf[8 : 8 + rows, at : at + step] = (total[:rows] * scale).astype(BF16).astype(F32)

    def conv(branch):
        first, last = branch * units, (branch + 1) * units
        count = taps.shape[1]
        summed = None
        for k in range(count):
            at = 8 - (count - 1) + k
            term = taps[branch, k : k + 1, :].astype(F32) * buf[at : at + rows, first:last]
            summed = term if summed is None else summed + term
        return summed

    hidden[...] = (silu(conv(0)) * conv(1)).astype(BF16)
    copies[-1].wait()
    for target, side in ((give, 1 - mine), (keep, mine)):
        for c in range(chips):
            at = pl.multiple_of((2 * c + side) * share, share)
            part = lax.dot_general(
                down[pl.ds(at, share), :], hidden[...], LAST, preferred_element_type=F32
            )
            target[c] = part.astype(BF16)


def exchange(parts, axis):
    return lax.all_to_all(parts, axis, split_axis=0, concat_axis=0, tiled=True)


def from_behind(value, axis):
    count = lax.axis_size(axis)
    return lax.ppermute(value, axis, [(source, source + 1) for source in range(count - 1)])


def swapped(value):
    return lax.ppermute(value, "core", [(0, 1), (1, 0)])


def pair_then_chips(kept, given):
    both = (kept.astype(F32) + swapped(given).astype(F32)).astype(BF16)
    return exchange(both, "x")


def local(
    residual,
    values,
    gate_input,
    group_keys,
    time_step,
    decay_rate,
    skip_gain,
    conv_values,
    conv_keys,
    mix_gain,
    out_weight,
    norm_gain,
    hidden_gate,
    hidden_up,
    hidden_conv,
    hidden_down,
):
    rows, cols = values.shape
    key_cols = group_keys.shape[1]
    last = rows // 8 - 1
    whole = lambda a: pl.BlockSpec(a.shape, lambda i: (0, 0))
    own_rows, tail = call(
        pack_kernel,
        [((hidden_gate.shape[0], 3 * hidden_gate.shape[1]), BF16), ((8, cols + key_cols), BF16)],
        grid=(1,),
        in_specs=[whole(hidden_gate), whole(hidden_up), whole(hidden_gate)]
        + [pl.BlockSpec((8, width), lambda i: (last, 0)) for width in (cols, key_cols)],
        grant=60,
        name="pack",
    )(hidden_gate, hidden_up, hidden_down.T, values, group_keys)
    weights = lax.all_gather(own_rows, SP, axis=0, tiled=True)
    chips = lax.axis_size("x")
    n_tp = chips * lax.axis_size("core")
    n_row = lax.axis_size(SP[1])
    features = residual.shape[0]
    units = hidden_gate.shape[1]
    before = from_behind(tail, SP)
    core = lax.axis_index("core").astype(jnp.int32).reshape(1)
    span = STATE_WIDE // n_row + STATE_NARROW // n_row + 8
    x, keys, run, delta, run_col, pay = call(
        state_kernel,
        [
            ((rows, cols), BF16),
            ((rows, key_cols), BF16),
            ((GROUP_HEADS, rows), F32),
            ((GROUP_HEADS, rows), F32),
            ((rows, GROUP_HEADS), F32),
            ((n_row, span, HALF), BF16),
        ],
        [((rows + 8, cols), F32), ((rows + 8, key_cols), F32)],
        in_specs=[VMEM, VMEM, VMEM, VMEM, SMEM, VMEM, VMEM],
        grant=60,
        name="span_state",
    )(
        values,
        group_keys,
        before,
        time_step,
        decay_rate,
        conv_values,
        conv_keys,
    )
    by_row = exchange(pay, SP[1])
    base, slope = call(
        inside_kernel, [((rows, cols), F32), ((rows, cols), F32)], name="inside_span"
    )(x, keys, run, delta, run_col, jnp.repeat(skip_gain, HEAD_SIZE).reshape(1, -1), gate_input)
    (sums,) = call(
        row_total_kernel, [((lax.axis_size(SP[0]), span, HALF), BF16)], name="row_total"
    )(by_row)
    totals = exchange(sums, SP[0])
    place = lax.axis_index(SP[0]).astype(jnp.int32).reshape(1)
    (starts,) = call(
        prefix_kernel,
        [((n_row, span, HALF), BF16)],
        in_specs=[
            pl.BlockSpec(memory_space=pltpu.SMEM),
            pl.BlockSpec(memory_space=pltpu.VMEM),
            pl.BlockSpec(memory_space=pltpu.VMEM),
        ],
        name="prefix",
    )(place, by_row, totals)
    carried = exchange(starts, SP[1])
    kept, given = call(
        apply_kernel,
        [((chips, rows + 16, features), BF16)] * 2,
        in_specs=[SMEM] + [VMEM] * 6,
        name="apply_project",
    )(core, base, slope, keys, carried, mix_gain.reshape(1, -1), out_weight)
    summed = pair_then_chips(kept, given)
    place_tp = lax.axis_index(("x", "core"))
    own_gain = lax.dynamic_slice_in_dim(norm_gain, place_tp * features, features, 0)
    lifted, tile, merged = call(
        functools.partial(merge_kernel, cols * n_tp),
        [((rows, features), BF16), ((8, features), BF16), ((features, rows), BF16)],
        name="merge",
    )(summed, residual, own_gain.reshape(1, -1))
    stream = jnp.concatenate([lifted, tile, from_behind(tile, SP)], axis=0)
    own_core = exchange(jnp.broadcast_to(stream, (chips, *stream.shape)), "x")
    other_core = swapped(own_core)
    step = 256
    kept, given = call(
        functools.partial(channel_kernel, features * n_tp),
        [((chips, features, rows), BF16)] * 2,
        [
            ((rows + 16, features * n_tp), BF16),
            ((2 * units // step, features * n_tp, step), BF16),
            ((features * n_tp, units), BF16),
            ((rows + 8, 2 * units), F32),
            ((rows, units), BF16),
        ],
        more_scratch=[pltpu.SemaphoreType.DMA((2 * units // step + 1,))],
        grant=24,
        in_specs=[SMEM, VMEM, VMEM, pl.BlockSpec(memory_space=pltpu.HBM), VMEM],
        name="channel_mixer",
    )(
        core, own_core, other_core, pltpu.with_memory_space_constraint(weights, pltpu.HBM), hidden_conv
    )
    got = pair_then_chips(kept, given)
    return (merged.astype(F32) + jnp.sum(got.astype(F32), axis=0)).astype(BF16)


def solution(mesh):
    split = Mesh(mesh.devices.reshape(8, 8, 4, 2), ("sp_0", "sp_1", "x", "core"))
    tp = ("x", "core")
    placed = (
        P(tp, SP),
        P(SP, tp),
        P(SP, tp),
        P(SP, tp),
        P(tp, SP),
        P(tp),
        P(tp),
        P(None, tp),
        P(None, tp),
        P(tp),
        P(tp, None),
        P(),
        P(SP, tp),
        P(SP, tp),
        P(None, None, tp),
        P(tp, SP),
    )
    return jax.shard_map(local, mesh=split, in_specs=placed, out_specs=P(tp, SP), check_vma=False)
```

```python
import functools

import jax
import jax.numpy as jnp
from jax import lax
from jax.experimental import pallas as pl
from jax.experimental.pallas import tpu as pltpu
from jax.sharding import Mesh
from jax.sharding import PartitionSpec as P

GROUP_HEADS = 8
HEAD_SIZE = 64
STATE_WIDE = 128
STATE_NARROW = 64
HALF = GROUP_HEADS // 2 * HEAD_SIZE
SP = ("sp_0", "sp_1")
NORM_FLOOR = 0.1
F32 = jnp.float32
BF16 = jnp.bfloat16
HIGHEST = lax.Precision.HIGHEST
LAST = (((1,), (1,)), ((), ()))
FIRST = (((0,), (0,)), ((), ()))


SMEM = pl.BlockSpec(memory_space=pltpu.SMEM)
VMEM = pl.BlockSpec(memory_space=pltpu.VMEM)


def call(kernel, outs, scratch=(), grant=12, more_scratch=(), **more):
    return pl.pallas_call(
        kernel,
        out_shape=[jax.ShapeDtypeStruct(shape, kind) for shape, kind in outs],
        scratch_shapes=[pltpu.VMEM(shape, kind) for shape, kind in scratch] + list(more_scratch),
        compiler_params=pltpu.CompilerParams(vmem_limit_bytes=grant << 20),
        **more,
    )


def pack_kernel(gate, up, down, values, keys, rows_out, tail_out):
    rows, units = gate.shape
    cols = values.shape[1]
    rows_out[:rows, :units] = gate[...]
    rows_out[:rows, units:] = up[...]
    rows_out[rows:, :units] = down[: rows // 2]
    rows_out[rows:, units:] = down[rows // 2 :]
    tail_out[:, :cols] = values[...]
    tail_out[:, cols:] = keys[...]


def silu(a):
    return a / (1.0 + jnp.exp(-a))


def pieces(row, count):
    found = []
    for _ in range(count):
        part = row.astype(BF16).astype(F32)
        found.append(part)
        row = row - part
    return found


def head_lanes(cols):
    rows = cols.shape[0]
    lane = lax.broadcasted_iota(jnp.int32, (rows, 2 * HEAD_SIZE), 1)
    both = [
        jnp.where(lane < HEAD_SIZE, cols[:, h : h + 1], cols[:, h + 1 : h + 2])
        for h in range(0, GROUP_HEADS, 2)
    ]
    return jnp.concatenate(both, axis=1)


def as_row(col):
    return jnp.transpose(jnp.broadcast_to(col, (col.shape[0], 128)))[0:1, :]


def as_col(row):
    return jnp.transpose(jnp.broadcast_to(row, (8, row.shape[1])))[:, 0:1]


def conv_silu(buf, taps, rows):
    count = taps.shape[0]
    total = taps[count - 1 : count, :].astype(F32) * buf[8 : 8 + rows, :]
    for k in range(count - 1):
        at = 8 - (count - 1) + k
        total = total + taps[k : k + 1, :].astype(F32) * buf[at : at + rows, :]
    return silu(total)


def state_kernel(
    values, keys, before, step, rate, taps_v, taps_k, x_out, key_out, run_out, delta_out, run_col, pay, vbuf, kbuf
):
    rows, cols = values.shape
    vbuf[0:8, :] = before[:, :cols].astype(F32)
    vbuf[8 : 8 + rows, :] = values[...].astype(F32)
    kbuf[0:8, :] = before[:, cols:].astype(F32)
    kbuf[8 : 8 + rows, :] = keys[...].astype(F32)
    x = conv_silu(vbuf, taps_v, rows)
    k = conv_silu(kbuf, taps_k, rows).astype(BF16)
    x_out[...] = x.astype(BF16)
    key_out[...] = k
    pre = step[...]
    delta = jnp.maximum(pre, 0.0) + jnp.log1p(jnp.exp(-jnp.abs(pre)))
    upper = lax.broadcasted_iota(jnp.int32, (rows, rows), 0) <= lax.broadcasted_iota(
        jnp.int32, (rows, rows), 1
    )
    head = lax.broadcasted_iota(jnp.int32, delta.shape, 0)
    rates = jnp.zeros(delta.shape, F32)
    for h in range(GROUP_HEADS):
        rates = jnp.where(head == h, rate[h], rates)
    run = jnp.dot(-rates * delta, upper.astype(F32), precision=HIGHEST, preferred_element_type=F32)
    run_out[...] = run
    delta_out[...] = delta
    run_t = jnp.transpose(run)
    run_col[...] = run_t
    end = run_t[rows - 1 : rows, :]
    to_end = jnp.exp(end - run_t) * jnp.transpose(delta)
    weighted = (x * head_lanes(to_end)).astype(BF16)
    wide = lax.dot_general(k[:, :STATE_WIDE], weighted[:, :HALF], FIRST, preferred_element_type=F32)
    narrow = lax.dot_general(
        k[:, 2 * STATE_WIDE :], weighted[:, HALF:], FIRST, preferred_element_type=F32
    )
    ends = head_lanes(jnp.broadcast_to(end, (8, GROUP_HEADS)))[0:1, :]
    marks = pieces(ends[:, :HALF], 3) + pieces(ends[:, HALF:], 3) + [jnp.zeros((2, HALF), F32)]
    count = pay.shape[0]
    w, n = STATE_WIDE // count, STATE_NARROW // count
    for c in range(count):
        part = [wide[c * w : (c + 1) * w], narrow[c * n : (c + 1) * n]] + marks
        pay[c] = jnp.concatenate(part, axis=0).astype(BF16)


def inside_kernel(x, keys, run, delta, run_col, skip, gate, base_out, slope_out):
    rows = x.shape[0]
    xs = x[...]
    k = keys[...]
    wide_end = 2 * STATE_WIDE
    score_w = lax.dot_general(k[:, STATE_WIDE:wide_end], k[:, :STATE_WIDE], LAST, preferred_element_type=F32)
    score_n = lax.dot_general(
        k[:, wide_end + STATE_NARROW :], k[:, wide_end : wide_end + STATE_NARROW], LAST, preferred_element_type=F32
    )
    keep = lax.broadcasted_iota(jnp.int32, (rows, rows), 0) >= lax.broadcasted_iota(
        jnp.int32, (rows, rows), 1
    )
    runs, deltas, cols = run[...], delta[...], run_col[...]
    outs = []
    for h in range(GROUP_HEADS):
        gap = jnp.where(keep, cols[:, h : h + 1] - runs[h : h + 1, :], -jnp.inf)
        score = score_w if h < GROUP_HEADS // 2 else score_n
        mixed = (score * (jnp.exp(gap) * deltas[h : h + 1, :])).astype(BF16)
        outs.append(
            jnp.dot(mixed, xs[:, h * HEAD_SIZE : (h + 1) * HEAD_SIZE], preferred_element_type=F32)
        )
    opened = silu(gate[...].astype(F32))
    direct = jnp.concatenate(outs, axis=1) + skip[...] * xs.astype(F32)
    base_out[...] = direct * opened
    slope_out[...] = head_lanes(jnp.exp(cols)) * opened


def span_parts(piece):
    w = STATE_WIDE // 8
    n = STATE_NARROW // 8
    state = piece[: w + n]
    at = w + n
    wide = piece[at : at + 1] + piece[at + 1 : at + 2] + piece[at + 2 : at + 3]
    narrow = piece[at + 3 : at + 4] + piece[at + 4 : at + 5] + piece[at + 5 : at + 6]
    return state, wide, narrow


def fade(wide, narrow):
    w = STATE_WIDE // 8
    n = STATE_NARROW // 8
    lanes = wide.shape[1]
    return jnp.concatenate(
        [
            jnp.broadcast_to(jnp.exp(wide), (w, lanes)),
            jnp.broadcast_to(jnp.exp(narrow), (n, lanes)),
        ],
        axis=0,
    )


def row_total_kernel(got, pay):
    count = got.shape[0]
    total = None
    for c in range(count):
        state, wide, narrow = span_parts(got[c].astype(F32))
        if total is None:
            total, log_w, log_n = state, wide, narrow
        else:
            total = total * fade(wide, narrow) + state
            log_w, log_n = log_w + wide, log_n + narrow
    marks = pieces(log_w, 3) + pieces(log_n, 3) + [jnp.zeros((2, log_w.shape[1]), F32)]
    piece = jnp.concatenate([total] + marks, axis=0).astype(BF16)
    for c in range(count):
        pay[c] = piece


def prefix_kernel(place, got, totals, pay):
    count = got.shape[0]
    mine = place[0]
    total = jnp.zeros((pay.shape[1] - 8, pay.shape[2]), F32)
    for c in range(totals.shape[0]):
        state, wide, narrow = span_parts(totals[c].astype(F32))
        total = jnp.where(c < mine, total * fade(wide, narrow) + state, total)
    pad = jnp.zeros((8, pay.shape[2]), F32)
    for c in range(count):
        pay[c] = jnp.concatenate([total, pad], axis=0).astype(BF16)
        state, wide, narrow = span_parts(got[c].astype(F32))
        total = total * fade(wide, narrow) + state


def apply_kernel(core, base, slope, keys, got, gain, weight, keep, give):
    count = got.shape[0]
    w = STATE_WIDE // count
    n = STATE_NARROW // count
    carried = [got[c].astype(F32) for c in range(count)]
    wide = jnp.concatenate([c[:w] for c in carried], axis=0).astype(BF16)
    narrow = jnp.concatenate([c[w : w + n] for c in carried], axis=0).astype(BF16)
    k = keys[...]
    wide_end = 2 * STATE_WIDE
    from_wide = jnp.dot(k[:, STATE_WIDE:wide_end], wide, preferred_element_type=F32)
    from_narrow = jnp.dot(k[:, wide_end + STATE_NARROW :], narrow, preferred_element_type=F32)
    gated = base[...] + slope[...] * jnp.concatenate([from_wide, from_narrow], axis=1)
    squares = as_row(jnp.sum(gated * gated, axis=1, keepdims=True))
    lanes = squares.shape[1]
    hi_lo = pieces(squares, 2)
    blank = jnp.zeros((2, lanes), F32)
    rest = jnp.zeros((12, lanes), F32)
    marks = jnp.concatenate(hi_lo + [blank, rest], axis=0).astype(BF16)
    given = jnp.concatenate([blank] + hi_lo + [rest], axis=0).astype(BF16)
    scaled = (gated * gain[...]).astype(BF16)
    rows, share = scaled.shape[0], keep.shape[2]
    mine = core[0]
    for target, side, mark in ((give, 1 - mine, given), (keep, mine, marks)):
        for c in range(target.shape[0]):
            at = pl.multiple_of((2 * c + side) * share, share)
            part = jnp.dot(scaled, weight[:, pl.ds(at, share)], preferred_element_type=F32)
            target[c, 0:rows, :] = part.astype(BF16)
            target[c, rows : rows + 16, :] = mark


def merge_kernel(channels, got, residual, gain, lifted_out, tile_out, merged_out):
    rows = residual.shape[1]
    total = got[0].astype(F32)
    for c in range(1, got.shape[0]):
        total = total + got[c].astype(F32)
    squares = jnp.sum(total[rows : rows + 8], axis=0, keepdims=True)
    inverse = as_col(lax.rsqrt(squares / channels + NORM_FLOOR))
    merged = jnp.transpose(residual[...].astype(F32)) + inverse * total[:rows]
    merged = merged.astype(BF16).astype(F32)
    merged_out[...] = jnp.transpose(merged).astype(BF16)
    own = as_row(jnp.sum(merged * merged, axis=1, keepdims=True))
    lifted = (merged * gain[...]).astype(BF16)
    lifted_out[...] = lifted
    edge = lifted[rows - 8 :, :].astype(F32)
    tile = pieces(own, 2) + [jnp.zeros((4, own.shape[1]), F32), edge[6:8]]
    tile_out[...] = jnp.concatenate(tile, axis=0).astype(BF16)


def channel_kernel(
    features, core, own, other, weights, taps, keep, give, lhs, wide, down, buf, hidden, total, sems
):
    chips, high, share = own.shape
    rows = high - 16
    units = hidden.shape[1]
    spans, each, _ = wide.shape
    half = down.shape[1]
    quarters = 4
    copies = []
    for first, last, target, count in ((0, each, wide, quarters), (each, each + half, down, 2)):
        step = spans // count
        for n in range(count):
            part = pl.ds(n * step, step)
            copies.append(
                pltpu.make_async_copy(
                    weights.at[part, first:last], target.at[part], sems.at[len(copies)]
                )
            )
    for copy in copies:
        copy.start()
    mine = core[0]
    marks = jnp.zeros((16, share), F32)
    for c in range(chips):
        first, second = own[c], other[c]
        marks = marks + first[rows:].astype(F32) + second[rows:].astype(F32)
        at = 2 * c * share
        lhs[:, at : at + share] = jnp.where(mine == 0, first, second)
        lhs[:, at + share : at + 2 * share] = jnp.where(mine == 0, second, first)

    def inverse_of(at):
        squares = marks[at : at + 1, :] + marks[at + 1 : at + 2, :]
        return as_col(lax.rsqrt(squares / features + NORM_FLOOR))

    scale, before = inverse_of(0), inverse_of(8)
    step = spans // quarters
    depth = step * each
    for n in range(quarters):
        copies[n].wait()
        block = wide[n * step : (n + 1) * step].reshape(depth, 2 * units)
        part = jnp.dot(
            lhs[:, n * depth : (n + 1) * depth], block, preferred_element_type=F32
        )
        if n == 0:
            total[...] = part
        elif n < quarters - 1:
            total[...] += part
        else:
            part = total[...] + part
            edge = part[rows + 8 :] * before[rows - 8 :, :]
            buf[0:8, :] = edge.astype(BF16).astype(F32)
            buf[8 : 8 + rows, :] = (part[:rows] * scale).astype(BF16).astype(F32)

    def conv(branch):
        first, last = branch * units, (branch + 1) * units
        count = taps.shape[1]
        summed = None
        for k in range(count):
            at = 8 - (count - 1) + k
            term = taps[branch, k : k + 1, :].astype(F32) * buf[at : at + rows, first:last]
            summed = term if summed is None else summed + term
        return summed

    hidden[...] = (silu(conv(0)) * conv(1)).astype(BF16)
    for copy in copies[quarters:]:
        copy.wait()
    step = share // each
    for target, side in ((give, 1 - mine), (keep, mine)):
        for c in range(chips):
            block = down[pl.ds((2 * c + side) * step, step)]
            block = jnp.concatenate([block[:, :, :units], block[:, :, units:]], axis=1)
            part = lax.dot_general(
                block.reshape(share, units), hidden[...], LAST, preferred_element_type=F32
            )
            target[c] = part.astype(BF16)


def finish_kernel(merged, got, out):
    total = merged[...].astype(F32)
    for c in range(got.shape[0]):
        total = total + got[c].astype(F32)
    out[...] = total.astype(BF16)


def exchange(parts, axis):
    return lax.all_to_all(parts, axis, split_axis=0, concat_axis=0, tiled=True)


def from_behind(value, axis):
    count = lax.axis_size(axis)
    return lax.ppermute(value, axis, [(source, source + 1) for source in range(count - 1)])


def swapped(value):
    return lax.ppermute(value, "core", [(0, 1), (1, 0)])


def pair_then_chips(kept, given):
    both = (kept.astype(F32) + swapped(given).astype(F32)).astype(BF16)
    return exchange(both, "x")


def local(
    residual,
    values,
    gate_input,
    group_keys,
    time_step,
    decay_rate,
    skip_gain,
    conv_values,
    conv_keys,
    mix_gain,
    out_weight,
    norm_gain,
    hidden_gate,
    hidden_up,
    hidden_conv,
    hidden_down,
):
    rows, cols = values.shape
    key_cols = group_keys.shape[1]
    last = rows // 8 - 1
    whole = lambda a: pl.BlockSpec(a.shape, lambda i: (0, 0))
    own_rows, tail = call(
        pack_kernel,
        [
            ((hidden_gate.shape[0] * 3 // 2, 2 * hidden_gate.shape[1]), BF16),
            ((8, cols + key_cols), BF16),
        ],
        grid=(1,),
        in_specs=[whole(hidden_gate), whole(hidden_up), whole(hidden_gate)]
        + [pl.BlockSpec((8, width), lambda i: (last, 0)) for width in (cols, key_cols)],
        grant=60,
        name="pack",
    )(hidden_gate, hidden_up, hidden_down.T, values, group_keys)
    weights = lax.all_gather(own_rows, SP, axis=0)
    chips = lax.axis_size("x")
    n_tp = chips * lax.axis_size("core")
    n_row = lax.axis_size(SP[1])
    features = residual.shape[0]
    units = hidden_gate.shape[1]
    before = from_behind(tail, SP)
    core = lax.axis_index("core").astype(jnp.int32).reshape(1)
    span = STATE_WIDE // n_row + STATE_NARROW // n_row + 8
    x, keys, run, delta, run_col, pay = call(
        state_kernel,
        [
            ((rows, cols), BF16),
            ((rows, key_cols), BF16),
            ((GROUP_HEADS, rows), F32),
            ((GROUP_HEADS, rows), F32),
            ((rows, GROUP_HEADS), F32),
            ((n_row, span, HALF), BF16),
        ],
        [((rows + 8, cols), F32), ((rows + 8, key_cols), F32)],
        in_specs=[VMEM, VMEM, VMEM, VMEM, SMEM, VMEM, VMEM],
        grant=60,
        name="span_state",
    )(
        values,
        group_keys,
        before,
        time_step,
        decay_rate,
        conv_values,
        conv_keys,
    )
    by_row = exchange(pay, SP[1])
    base, slope = call(
        inside_kernel, [((rows, cols), F32), ((rows, cols), F32)], name="inside_span"
    )(x, keys, run, delta, run_col, jnp.repeat(skip_gain, HEAD_SIZE).reshape(1, -1), gate_input)
    (sums,) = call(
        row_total_kernel, [((lax.axis_size(SP[0]), span, HALF), BF16)], name="row_total"
    )(by_row)
    totals = exchange(sums, SP[0])
    place = lax.axis_index(SP[0]).astype(jnp.int32).reshape(1)
    (starts,) = call(
        prefix_kernel,
        [((n_row, span, HALF), BF16)],
        in_specs=[
            pl.BlockSpec(memory_space=pltpu.SMEM),
            pl.BlockSpec(memory_space=pltpu.VMEM),
            pl.BlockSpec(memory_space=pltpu.VMEM),
        ],
        name="prefix",
    )(place, by_row, totals)
    carried = exchange(starts, SP[1])
    kept, given = call(
        apply_kernel,
        [((chips, rows + 16, features), BF16)] * 2,
        in_specs=[SMEM] + [VMEM] * 6,
        name="apply_project",
    )(core, base, slope, keys, carried, mix_gain.reshape(1, -1), out_weight)
    summed = pair_then_chips(kept, given)
    place_tp = lax.axis_index(("x", "core"))
    own_gain = lax.dynamic_slice_in_dim(norm_gain, place_tp * features, features, 0)
    lifted, tile, merged = call(
        functools.partial(merge_kernel, cols * n_tp),
        [((rows, features), BF16), ((8, features), BF16), ((features, rows), BF16)],
        name="merge",
    )(summed, residual, own_gain.reshape(1, -1))
    stream = jnp.concatenate([lifted, tile, from_behind(tile, SP)], axis=0)
    own_core = exchange(jnp.broadcast_to(stream, (chips, *stream.shape)), "x")
    other_core = swapped(own_core)
    spans, each = weights.shape[0], hidden_gate.shape[0]
    kept, given = call(
        functools.partial(channel_kernel, features * n_tp),
        [((chips, features, rows), BF16)] * 2,
        [
            ((rows + 16, features * n_tp), BF16),
            ((spans, each, 2 * units), BF16),
            ((spans, each // 2, 2 * units), BF16),
            ((rows + 8, 2 * units), F32),
            ((rows, units), BF16),
            ((rows + 16, 2 * units), F32),
        ],
        more_scratch=[pltpu.SemaphoreType.DMA((6,))],
        grant=24,
        in_specs=[SMEM, VMEM, VMEM, pl.BlockSpec(memory_space=pltpu.HBM), VMEM],
        name="channel_mixer",
    )(
        core, own_core, other_core, pltpu.with_memory_space_constraint(weights, pltpu.HBM), hidden_conv
    )
    got = pair_then_chips(kept, given)
    (out,) = call(finish_kernel, [((features, rows), BF16)], name="finish")(merged, got)
    return out


def solution(mesh):
    split = Mesh(mesh.devices.reshape(8, 8, 4, 2), ("sp_0", "sp_1", "x", "core"))
    tp = ("x", "core")
    placed = (
        P(tp, SP),
        P(SP, tp),
        P(SP, tp),
        P(SP, tp),
        P(tp, SP),
        P(tp),
        P(tp),
        P(None, tp),
        P(None, tp),
        P(tp),
        P(tp, None),
        P(),
        P(SP, tp),
        P(SP, tp),
        P(None, None, tp),
        P(tp, SP),
    )
    return jax.shard_map(local, mesh=split, in_specs=placed, out_specs=P(tp, SP), check_vma=False)
```

```python
import functools

import jax
import jax.numpy as jnp
from jax import lax
from jax.experimental import pallas as pl
from jax.experimental.pallas import tpu as pltpu
from jax.sharding import Mesh
from jax.sharding import PartitionSpec as P

GROUP_HEADS = 8
HEAD_SIZE = 64
STATE_WIDE = 128
STATE_NARROW = 64
HALF = GROUP_HEADS // 2 * HEAD_SIZE
SP = ("sp_0", "sp_1")
NORM_FLOOR = 0.1
F32 = jnp.float32
BF16 = jnp.bfloat16
HIGHEST = lax.Precision.HIGHEST
LAST = (((1,), (1,)), ((), ()))
FIRST = (((0,), (0,)), ((), ()))


SMEM = pl.BlockSpec(memory_space=pltpu.SMEM)
VMEM = pl.BlockSpec(memory_space=pltpu.VMEM)


def call(kernel, outs, scratch=(), grant=12, more_scratch=(), **more):
    return pl.pallas_call(
        kernel,
        out_shape=[jax.ShapeDtypeStruct(shape, kind) for shape, kind in outs],
        scratch_shapes=[pltpu.VMEM(shape, kind) for shape, kind in scratch] + list(more_scratch),
        compiler_params=pltpu.CompilerParams(vmem_limit_bytes=grant << 20),
        **more,
    )


def pack_kernel(gate, up, down, values, keys, rows_out, tail_out):
    rows, units = gate.shape
    cols = values.shape[1]
    rows_out[:rows, :units] = gate[...]
    rows_out[:rows, units:] = up[...]
    rows_out[rows:, :units] = down[: rows // 2]
    rows_out[rows:, units:] = down[rows // 2 :]
    tail_out[:, :cols] = values[...]
    tail_out[:, cols:] = keys[...]


def silu(a):
    return a / (1.0 + jnp.exp(-a))


def pieces(row, count):
    found = []
    for _ in range(count):
        part = row.astype(BF16).astype(F32)
        found.append(part)
        row = row - part
    return found


def head_lanes(cols):
    rows = cols.shape[0]
    lane = lax.broadcasted_iota(jnp.int32, (rows, 2 * HEAD_SIZE), 1)
    both = [
        jnp.where(lane < HEAD_SIZE, cols[:, h : h + 1], cols[:, h + 1 : h + 2])
        for h in range(0, GROUP_HEADS, 2)
    ]
    return jnp.concatenate(both, axis=1)


def as_row(col):
    return jnp.transpose(jnp.broadcast_to(col, (col.shape[0], 128)))[0:1, :]


def as_col(row):
    return jnp.transpose(jnp.broadcast_to(row, (8, row.shape[1])))[:, 0:1]


def conv_silu(buf, taps, rows):
    count = taps.shape[0]
    total = taps[count - 1 : count, :].astype(F32) * buf[8 : 8 + rows, :]
    for k in range(count - 1):
        at = 8 - (count - 1) + k
        total = total + taps[k : k + 1, :].astype(F32) * buf[at : at + rows, :]
    return silu(total)


def state_kernel(
    values, keys, before, step, rate, taps_v, taps_k, x_out, key_out, run_out, delta_out, run_col, pay, vbuf, kbuf
):
    rows, cols = values.shape
    vbuf[0:8, :] = before[:, :cols].astype(F32)
    vbuf[8 : 8 + rows, :] = values[...].astype(F32)
    kbuf[0:8, :] = before[:, cols:].astype(F32)
    kbuf[8 : 8 + rows, :] = keys[...].astype(F32)
    x = conv_silu(vbuf, taps_v, rows)
    k = conv_silu(kbuf, taps_k, rows).astype(BF16)
    x_out[...] = x.astype(BF16)
    key_out[...] = k
    pre = step[...]
    delta = jnp.maximum(pre, 0.0) + jnp.log1p(jnp.exp(-jnp.abs(pre)))
    upper = lax.broadcasted_iota(jnp.int32, (rows, rows), 0) <= lax.broadcasted_iota(
        jnp.int32, (rows, rows), 1
    )
    head = lax.broadcasted_iota(jnp.int32, delta.shape, 0)
    rates = jnp.zeros(delta.shape, F32)
    for h in range(GROUP_HEADS):
        rates = jnp.where(head == h, rate[h], rates)
    run = jnp.dot(-rates * delta, upper.astype(F32), precision=HIGHEST, preferred_element_type=F32)
    run_out[...] = run
    delta_out[...] = delta
    run_t = jnp.transpose(run)
    run_col[...] = run_t
    end = run_t[rows - 1 : rows, :]
    to_end = jnp.exp(end - run_t) * jnp.transpose(delta)
    weighted = (x * head_lanes(to_end)).astype(BF16)
    wide = lax.dot_general(k[:, :STATE_WIDE], weighted[:, :HALF], FIRST, preferred_element_type=F32)
    narrow = lax.dot_general(
        k[:, 2 * STATE_WIDE :], weighted[:, HALF:], FIRST, preferred_element_type=F32
    )
    ends = head_lanes(jnp.broadcast_to(end, (8, GROUP_HEADS)))[0:1, :]
    marks = pieces(ends[:, :HALF], 3) + pieces(ends[:, HALF:], 3) + [jnp.zeros((2, HALF), F32)]
    count = pay.shape[0]
    w, n = STATE_WIDE // count, STATE_NARROW // count
    for c in range(count):
        part = [wide[c * w : (c + 1) * w], narrow[c * n : (c + 1) * n]] + marks
        pay[c] = jnp.concatenate(part, axis=0).astype(BF16)


def inside_kernel(x, keys, run, delta, run_col, skip, gate, base_out, slope_out):
    rows = x.shape[0]
    xs = x[...]
    k = keys[...]
    wide_end = 2 * STATE_WIDE
    score_w = lax.dot_general(k[:, STATE_WIDE:wide_end], k[:, :STATE_WIDE], LAST, preferred_element_type=F32)
    score_n = lax.dot_general(
        k[:, wide_end + STATE_NARROW :], k[:, wide_end : wide_end + STATE_NARROW], LAST, preferred_element_type=F32
    )
    keep = lax.broadcasted_iota(jnp.int32, (rows, rows), 0) >= lax.broadcasted_iota(
        jnp.int32, (rows, rows), 1
    )
    runs, deltas, cols = run[...], delta[...], run_col[...]
    outs = []
    for h in range(GROUP_HEADS):
        gap = jnp.where(keep, cols[:, h : h + 1] - runs[h : h + 1, :], -jnp.inf)
        score = score_w if h < GROUP_HEADS // 2 else score_n
        mixed = (score * (jnp.exp(gap) * deltas[h : h + 1, :])).astype(BF16)
        outs.append(
            jnp.dot(mixed, xs[:, h * HEAD_SIZE : (h + 1) * HEAD_SIZE], preferred_element_type=F32)
        )
    opened = silu(gate[...].astype(F32))
    direct = jnp.concatenate(outs, axis=1) + skip[...] * xs.astype(F32)
    base_out[...] = direct * opened
    slope_out[...] = head_lanes(jnp.exp(cols)) * opened


def span_parts(piece):
    w = STATE_WIDE // 8
    n = STATE_NARROW // 8
    state = piece[: w + n]
    at = w + n
    wide = piece[at : at + 1] + piece[at + 1 : at + 2] + piece[at + 2 : at + 3]
    narrow = piece[at + 3 : at + 4] + piece[at + 4 : at + 5] + piece[at + 5 : at + 6]
    return state, wide, narrow


def fade(wide, narrow):
    w = STATE_WIDE // 8
    n = STATE_NARROW // 8
    lanes = wide.shape[1]
    return jnp.concatenate(
        [
            jnp.broadcast_to(jnp.exp(wide), (w, lanes)),
            jnp.broadcast_to(jnp.exp(narrow), (n, lanes)),
        ],
        axis=0,
    )


def row_total_kernel(got, pay):
    count = got.shape[0]
    total = None
    for c in range(count):
        state, wide, narrow = span_parts(got[c].astype(F32))
        if total is None:
            total, log_w, log_n = state, wide, narrow
        else:
            total = total * fade(wide, narrow) + state
            log_w, log_n = log_w + wide, log_n + narrow
    marks = pieces(log_w, 3) + pieces(log_n, 3) + [jnp.zeros((2, log_w.shape[1]), F32)]
    piece = jnp.concatenate([total] + marks, axis=0).astype(BF16)
    for c in range(count):
        pay[c] = piece


def prefix_kernel(place, got, totals, pay):
    count = got.shape[0]
    mine = place[0]
    total = jnp.zeros((pay.shape[1] - 8, pay.shape[2]), F32)
    for c in range(totals.shape[0]):
        state, wide, narrow = span_parts(totals[c].astype(F32))
        total = jnp.where(c < mine, total * fade(wide, narrow) + state, total)
    pad = jnp.zeros((8, pay.shape[2]), F32)
    for c in range(count):
        pay[c] = jnp.concatenate([total, pad], axis=0).astype(BF16)
        state, wide, narrow = span_parts(got[c].astype(F32))
        total = total * fade(wide, narrow) + state


def apply_kernel(core, base, slope, keys, got, gain, weight, keep, give):
    count = got.shape[0]
    w = STATE_WIDE // count
    n = STATE_NARROW // count
    carried = [got[c].astype(F32) for c in range(count)]
    wide = jnp.concatenate([c[:w] for c in carried], axis=0).astype(BF16)
    narrow = jnp.concatenate([c[w : w + n] for c in carried], axis=0).astype(BF16)
    k = keys[...]
    wide_end = 2 * STATE_WIDE
    from_wide = jnp.dot(k[:, STATE_WIDE:wide_end], wide, preferred_element_type=F32)
    from_narrow = jnp.dot(k[:, wide_end + STATE_NARROW :], narrow, preferred_element_type=F32)
    gated = base[...] + slope[...] * jnp.concatenate([from_wide, from_narrow], axis=1)
    squares = as_row(jnp.sum(gated * gated, axis=1, keepdims=True))
    lanes = squares.shape[1]
    hi_lo = pieces(squares, 2)
    blank = jnp.zeros((2, lanes), F32)
    rest = jnp.zeros((12, lanes), F32)
    marks = jnp.concatenate(hi_lo + [blank, rest], axis=0).astype(BF16)
    given = jnp.concatenate([blank] + hi_lo + [rest], axis=0).astype(BF16)
    scaled = (gated * gain[...]).astype(BF16)
    rows, share = scaled.shape[0], keep.shape[2]
    mine = core[0]
    for target, side, mark in ((give, 1 - mine, given), (keep, mine, marks)):
        for c in range(target.shape[0]):
            at = pl.multiple_of((2 * c + side) * share, share)
            part = jnp.dot(scaled, weight[:, pl.ds(at, share)], preferred_element_type=F32)
            target[c, 0:rows, :] = part.astype(BF16)
            target[c, rows : rows + 16, :] = mark


def merge_kernel(channels, got, residual, gain, lifted_out, tile_out, merged_out):
    rows = residual.shape[1]
    total = got[0].astype(F32)
    for c in range(1, got.shape[0]):
        total = total + got[c].astype(F32)
    squares = jnp.sum(total[rows : rows + 8], axis=0, keepdims=True)
    inverse = as_col(lax.rsqrt(squares / channels + NORM_FLOOR))
    merged = jnp.transpose(residual[...].astype(F32)) + inverse * total[:rows]
    merged = merged.astype(BF16).astype(F32)
    merged_out[...] = jnp.transpose(merged).astype(BF16)
    own = as_row(jnp.sum(merged * merged, axis=1, keepdims=True))
    lifted = (merged * gain[...]).astype(BF16)
    lifted_out[...] = lifted
    edge = lifted[rows - 8 :, :].astype(F32)
    tile = pieces(own, 2) + [jnp.zeros((4, own.shape[1]), F32), edge[6:8]]
    tile_out[...] = jnp.concatenate(tile, axis=0).astype(BF16)


def channel_kernel(
    features, core, own, other, weights, taps, keep, give, lhs, wide, down, buf, hidden, total, sems
):
    chips, high, share = own.shape
    rows = high - 16
    units = hidden.shape[1]
    spans, each, _ = wide.shape
    half = down.shape[1]
    quarters = 4
    copies = []
    for first, last, target, count in ((0, each, wide, quarters), (each, each + half, down, 2)):
        step = spans // count
        for n in range(count):
            part = pl.ds(n * step, step)
            copies.append(
                pltpu.make_async_copy(
                    weights.at[part, first:last], target.at[part], sems.at[len(copies)]
                )
            )
    for copy in copies:
        copy.start()
    mine, chip = core[0], core[1]
    odd = chip % 2
    near = chip + 1 - 2 * odd
    back = (chip + 2 * odd + 3) % 4
    across = (chip + 2) % 4
    marks = jnp.zeros((16, share), F32)
    for c in range(chips):
        first, second = own[c], other[c]
        marks = marks + first[rows:].astype(F32) + second[rows:].astype(F32)
        at = 2 * c * share
        lhs[:, at : at + share] = jnp.where(mine == 0, first, second)
        lhs[:, at + share : at + 2 * share] = jnp.where(mine == 0, second, first)

    def inverse_of(at):
        squares = marks[at : at + 1, :] + marks[at + 1 : at + 2, :]
        return as_col(lax.rsqrt(squares / features + NORM_FLOOR))

    scale, before = inverse_of(0), inverse_of(8)
    step = spans // quarters
    depth = step * each
    for n in range(quarters):
        copies[n].wait()
        block = wide[n * step : (n + 1) * step].reshape(depth, 2 * units)
        part = jnp.dot(
            lhs[:, n * depth : (n + 1) * depth], block, preferred_element_type=F32
        )
        if n == 0:
            total[...] = part
        elif n < quarters - 1:
            total[...] += part
        else:
            part = total[...] + part
            edge = part[rows + 8 :] * before[rows - 8 :, :]
            buf[0:8, :] = edge.astype(BF16).astype(F32)
            buf[8 : 8 + rows, :] = (part[:rows] * scale).astype(BF16).astype(F32)

    def conv(branch):
        first, last = branch * units, (branch + 1) * units
        count = taps.shape[1]
        summed = None
        for k in range(count):
            at = 8 - (count - 1) + k
            term = taps[branch, k : k + 1, :].astype(F32) * buf[at : at + rows, first:last]
            summed = term if summed is None else summed + term
        return summed

    hidden[...] = (silu(conv(0)) * conv(1)).astype(BF16)
    for copy in copies[quarters:]:
        copy.wait()
    step = share // each
    for target, side in ((give, 1 - mine), (keep, mine)):
        first = jnp.where(side == 0, near, back)
        second = near + back - first
        for c, block in enumerate((chip, second, first, across)):
            block = down[pl.ds((2 * block + side) * step, step)]
            block = jnp.concatenate([block[:, :, :units], block[:, :, units:]], axis=1)
            part = lax.dot_general(
                block.reshape(share, units), hidden[...], LAST, preferred_element_type=F32
            )
            target[c] = part.astype(BF16)


def finish_kernel(merged, kept, swapped_in, first_in, second_in, out):
    total = merged[...].astype(F32) + kept[0].astype(F32) + swapped_in[0].astype(F32)
    total = total + first_in[0].astype(F32) + second_in[...].astype(F32)
    out[...] = total.astype(BF16)


def halved(kept, given, merged):
    near = [(0, 1), (1, 0), (2, 3), (3, 2)]
    back = [(0, 3), (3, 0), (1, 2), (2, 1)]
    rounds = [
        [(2 * a, 2 * b) for a, b in even] + [(2 * a + 1, 2 * b + 1) for a, b in odd]
        for even, odd in ((near, back), (back, near))
    ]
    tp = ("x", "core")
    got = swapped(given)
    sent = (kept[2:].astype(F32) + got[2:].astype(F32)).astype(BF16)
    first = lax.ppermute(sent, tp, rounds[0])
    sent = kept[1].astype(F32) + got[1].astype(F32) + first[1].astype(F32)
    second = lax.ppermute(sent.astype(BF16), tp, rounds[1])
    (out,) = call(finish_kernel, [(merged.shape, BF16)], name="finish")(
        merged, kept, got, first, second
    )
    return out


def exchange(parts, axis):
    return lax.all_to_all(parts, axis, split_axis=0, concat_axis=0, tiled=True)


def from_behind(value, axis):
    count = lax.axis_size(axis)
    return lax.ppermute(value, axis, [(source, source + 1) for source in range(count - 1)])


def swapped(value):
    return lax.ppermute(value, "core", [(0, 1), (1, 0)])


def pair_then_chips(kept, given):
    both = (kept.astype(F32) + swapped(given).astype(F32)).astype(BF16)
    return exchange(both, "x")


def local(
    residual,
    values,
    gate_input,
    group_keys,
    time_step,
    decay_rate,
    skip_gain,
    conv_values,
    conv_keys,
    mix_gain,
    out_weight,
    norm_gain,
    hidden_gate,
    hidden_up,
    hidden_conv,
    hidden_down,
):
    rows, cols = values.shape
    key_cols = group_keys.shape[1]
    last = rows // 8 - 1
    whole = lambda a: pl.BlockSpec(a.shape, lambda i: (0, 0))
    own_rows, tail = call(
        pack_kernel,
        [
            ((hidden_gate.shape[0] * 3 // 2, 2 * hidden_gate.shape[1]), BF16),
            ((8, cols + key_cols), BF16),
        ],
        grid=(1,),
        in_specs=[whole(hidden_gate), whole(hidden_up), whole(hidden_gate)]
        + [pl.BlockSpec((8, width), lambda i: (last, 0)) for width in (cols, key_cols)],
        grant=60,
        name="pack",
    )(hidden_gate, hidden_up, hidden_down.T, values, group_keys)
    weights = lax.all_gather(own_rows, SP, axis=0)
    chips = lax.axis_size("x")
    n_tp = chips * lax.axis_size("core")
    n_row = lax.axis_size(SP[1])
    features = residual.shape[0]
    units = hidden_gate.shape[1]
    before = from_behind(tail, SP)
    core = jnp.stack([lax.axis_index("core"), lax.axis_index("x")]).astype(jnp.int32)
    span = STATE_WIDE // n_row + STATE_NARROW // n_row + 8
    x, keys, run, delta, run_col, pay = call(
        state_kernel,
        [
            ((rows, cols), BF16),
            ((rows, key_cols), BF16),
            ((GROUP_HEADS, rows), F32),
            ((GROUP_HEADS, rows), F32),
            ((rows, GROUP_HEADS), F32),
            ((n_row, span, HALF), BF16),
        ],
        [((rows + 8, cols), F32), ((rows + 8, key_cols), F32)],
        in_specs=[VMEM, VMEM, VMEM, VMEM, SMEM, VMEM, VMEM],
        grant=60,
        name="span_state",
    )(
        values,
        group_keys,
        before,
        time_step,
        decay_rate,
        conv_values,
        conv_keys,
    )
    by_row = exchange(pay, SP[1])
    base, slope = call(
        inside_kernel, [((rows, cols), F32), ((rows, cols), F32)], name="inside_span"
    )(x, keys, run, delta, run_col, jnp.repeat(skip_gain, HEAD_SIZE).reshape(1, -1), gate_input)
    (sums,) = call(
        row_total_kernel, [((lax.axis_size(SP[0]), span, HALF), BF16)], name="row_total"
    )(by_row)
    totals = exchange(sums, SP[0])
    place = lax.axis_index(SP[0]).astype(jnp.int32).reshape(1)
    (starts,) = call(
        prefix_kernel,
        [((n_row, span, HALF), BF16)],
        in_specs=[
            pl.BlockSpec(memory_space=pltpu.SMEM),
            pl.BlockSpec(memory_space=pltpu.VMEM),
            pl.BlockSpec(memory_space=pltpu.VMEM),
        ],
        name="prefix",
    )(place, by_row, totals)
    carried = exchange(starts, SP[1])
    kept, given = call(
        apply_kernel,
        [((chips, rows + 16, features), BF16)] * 2,
        in_specs=[SMEM] + [VMEM] * 6,
        name="apply_project",
    )(core, base, slope, keys, carried, mix_gain.reshape(1, -1), out_weight)
    summed = pair_then_chips(kept, given)
    place_tp = lax.axis_index(("x", "core"))
    own_gain = lax.dynamic_slice_in_dim(norm_gain, place_tp * features, features, 0)
    lifted, tile, merged = call(
        functools.partial(merge_kernel, cols * n_tp),
        [((rows, features), BF16), ((8, features), BF16), ((features, rows), BF16)],
        name="merge",
    )(summed, residual, own_gain.reshape(1, -1))
    stream = jnp.concatenate([lifted, tile, from_behind(tile, SP)], axis=0)
    own_core = exchange(jnp.broadcast_to(stream, (chips, *stream.shape)), "x")
    other_core = swapped(own_core)
    spans, each = weights.shape[0], hidden_gate.shape[0]
    kept, given = call(
        functools.partial(channel_kernel, features * n_tp),
        [((chips, features, rows), BF16)] * 2,
        [
            ((rows + 16, features * n_tp), BF16),
            ((spans, each, 2 * units), BF16),
            ((spans, each // 2, 2 * units), BF16),
            ((rows + 8, 2 * units), F32),
            ((rows, units), BF16),
            ((rows + 16, 2 * units), F32),
        ],
        more_scratch=[pltpu.SemaphoreType.DMA((6,))],
        grant=24,
        in_specs=[SMEM, VMEM, VMEM, pl.BlockSpec(memory_space=pltpu.HBM), VMEM],
        name="channel_mixer",
    )(
        core, own_core, other_core, pltpu.with_memory_space_constraint(weights, pltpu.HBM), hidden_conv
    )
    return halved(kept, given, merged)


def solution(mesh):
    split = Mesh(mesh.devices.reshape(8, 8, 4, 2), ("sp_0", "sp_1", "x", "core"))
    tp = ("x", "core")
    placed = (
        P(tp, SP),
        P(SP, tp),
        P(SP, tp),
        P(SP, tp),
        P(tp, SP),
        P(tp),
        P(tp),
        P(None, tp),
        P(None, tp),
        P(tp),
        P(tp, None),
        P(),
        P(SP, tp),
        P(SP, tp),
        P(None, None, tp),
        P(tp, SP),
    )
    return jax.shard_map(local, mesh=split, in_specs=placed, out_specs=P(tp, SP), check_vma=False)
```

```python
import functools

import jax
import jax.numpy as jnp
from jax import lax
from jax.experimental import pallas as pl
from jax.experimental.pallas import tpu as pltpu
from jax.sharding import Mesh
from jax.sharding import PartitionSpec as P

GROUP_HEADS = 8
HEAD_SIZE = 64
STATE_WIDE = 128
STATE_NARROW = 64
HALF = GROUP_HEADS // 2 * HEAD_SIZE
SP = ("sp_0", "sp_1")
NORM_FLOOR = 0.1
F32 = jnp.float32
BF16 = jnp.bfloat16
HIGHEST = lax.Precision.HIGHEST
LAST = (((1,), (1,)), ((), ()))
FIRST = (((0,), (0,)), ((), ()))


SMEM = pl.BlockSpec(memory_space=pltpu.SMEM)
VMEM = pl.BlockSpec(memory_space=pltpu.VMEM)


def call(kernel, outs, scratch=(), grant=12, more_scratch=(), **more):
    return pl.pallas_call(
        kernel,
        out_shape=[jax.ShapeDtypeStruct(shape, kind) for shape, kind in outs],
        scratch_shapes=[pltpu.VMEM(shape, kind) for shape, kind in scratch] + list(more_scratch),
        compiler_params=pltpu.CompilerParams(vmem_limit_bytes=grant << 20),
        **more,
    )


def pack_kernel(gate, up, down, values, keys, rows_out, tail_out):
    rows, units = gate.shape
    cols = values.shape[1]
    rows_out[:rows, :units] = gate[...]
    rows_out[:rows, units:] = up[...]
    rows_out[rows:, :units] = down[: rows // 2]
    rows_out[rows:, units:] = down[rows // 2 :]
    tail_out[:, :cols] = values[...]
    tail_out[:, cols:] = keys[...]


def silu(a):
    return a / (1.0 + jnp.exp(-a))


def pieces(row, count):
    found = []
    for _ in range(count):
        part = row.astype(BF16).astype(F32)
        found.append(part)
        row = row - part
    return found


def head_lanes(cols):
    rows = cols.shape[0]
    lane = lax.broadcasted_iota(jnp.int32, (rows, 2 * HEAD_SIZE), 1)
    both = [
        jnp.where(lane < HEAD_SIZE, cols[:, h : h + 1], cols[:, h + 1 : h + 2])
        for h in range(0, GROUP_HEADS, 2)
    ]
    return jnp.concatenate(both, axis=1)


def as_row(col):
    return jnp.transpose(jnp.broadcast_to(col, (col.shape[0], 128)))[0:1, :]


def as_col(row):
    return jnp.transpose(jnp.broadcast_to(row, (8, row.shape[1])))[:, 0:1]


def conv_silu(buf, taps, rows):
    count = taps.shape[0]
    total = taps[count - 1 : count, :].astype(F32) * buf[8 : 8 + rows, :]
    for k in range(count - 1):
        at = 8 - (count - 1) + k
        total = total + taps[k : k + 1, :].astype(F32) * buf[at : at + rows, :]
    return silu(total)


def state_kernel(
    values, keys, before, step, rate, taps_v, taps_k, x_out, key_out, run_out, delta_out, run_col, pay, vbuf, kbuf
):
    rows, cols = values.shape
    vbuf[0:8, :] = before[:, :cols].astype(F32)
    vbuf[8 : 8 + rows, :] = values[...].astype(F32)
    kbuf[0:8, :] = before[:, cols:].astype(F32)
    kbuf[8 : 8 + rows, :] = keys[...].astype(F32)
    x = conv_silu(vbuf, taps_v, rows)
    k = conv_silu(kbuf, taps_k, rows).astype(BF16)
    x_out[...] = x.astype(BF16)
    key_out[...] = k
    pre = step[...]
    delta = jnp.maximum(pre, 0.0) + jnp.log1p(jnp.exp(-jnp.abs(pre)))
    upper = lax.broadcasted_iota(jnp.int32, (rows, rows), 0) <= lax.broadcasted_iota(
        jnp.int32, (rows, rows), 1
    )
    head = lax.broadcasted_iota(jnp.int32, delta.shape, 0)
    rates = jnp.zeros(delta.shape, F32)
    for h in range(GROUP_HEADS):
        rates = jnp.where(head == h, rate[h], rates)
    run = jnp.dot(-rates * delta, upper.astype(F32), precision=HIGHEST, preferred_element_type=F32)
    run_out[...] = run
    delta_out[...] = delta
    run_t = jnp.transpose(run)
    run_col[...] = run_t
    end = run_t[rows - 1 : rows, :]
    to_end = jnp.exp(end - run_t) * jnp.transpose(delta)
    weighted = (x * head_lanes(to_end)).astype(BF16)
    wide = lax.dot_general(k[:, :STATE_WIDE], weighted[:, :HALF], FIRST, preferred_element_type=F32)
    narrow = lax.dot_general(
        k[:, 2 * STATE_WIDE :], weighted[:, HALF:], FIRST, preferred_element_type=F32
    )
    ends = head_lanes(jnp.broadcast_to(end, (8, GROUP_HEADS)))[0:1, :]
    marks = pieces(ends[:, :HALF], 3) + pieces(ends[:, HALF:], 3) + [jnp.zeros((2, HALF), F32)]
    count = pay.shape[0]
    w, n = STATE_WIDE // count, STATE_NARROW // count
    for c in range(count):
        part = [wide[c * w : (c + 1) * w], narrow[c * n : (c + 1) * n]] + marks
        pay[c] = jnp.concatenate(part, axis=0).astype(BF16)


def inside_kernel(x, keys, run, delta, run_col, skip, gate, base_out, slope_out):
    rows = x.shape[0]
    xs = x[...]
    k = keys[...]
    wide_end = 2 * STATE_WIDE
    score_w = lax.dot_general(k[:, STATE_WIDE:wide_end], k[:, :STATE_WIDE], LAST, preferred_element_type=F32)
    score_n = lax.dot_general(
        k[:, wide_end + STATE_NARROW :], k[:, wide_end : wide_end + STATE_NARROW], LAST, preferred_element_type=F32
    )
    keep = lax.broadcasted_iota(jnp.int32, (rows, rows), 0) >= lax.broadcasted_iota(
        jnp.int32, (rows, rows), 1
    )
    runs, deltas, cols = run[...], delta[...], run_col[...]
    outs = []
    for h in range(GROUP_HEADS):
        gap = jnp.where(keep, cols[:, h : h + 1] - runs[h : h + 1, :], -jnp.inf)
        score = score_w if h < GROUP_HEADS // 2 else score_n
        mixed = (score * (jnp.exp(gap) * deltas[h : h + 1, :])).astype(BF16)
        outs.append(
            jnp.dot(mixed, xs[:, h * HEAD_SIZE : (h + 1) * HEAD_SIZE], preferred_element_type=F32)
        )
    opened = silu(gate[...].astype(F32))
    direct = jnp.concatenate(outs, axis=1) + skip[...] * xs.astype(F32)
    base_out[...] = direct * opened
    slope_out[...] = head_lanes(jnp.exp(cols)) * opened


def span_parts(piece):
    w = STATE_WIDE // 8
    n = STATE_NARROW // 8
    state = piece[: w + n]
    at = w + n
    wide = piece[at : at + 1] + piece[at + 1 : at + 2] + piece[at + 2 : at + 3]
    narrow = piece[at + 3 : at + 4] + piece[at + 4 : at + 5] + piece[at + 5 : at + 6]
    return state, wide, narrow


def fade(wide, narrow):
    w = STATE_WIDE // 8
    n = STATE_NARROW // 8
    lanes = wide.shape[1]
    return jnp.concatenate(
        [
            jnp.broadcast_to(jnp.exp(wide), (w, lanes)),
            jnp.broadcast_to(jnp.exp(narrow), (n, lanes)),
        ],
        axis=0,
    )


def row_total_kernel(got, pay):
    count = got.shape[0]
    total = None
    for c in range(count):
        state, wide, narrow = span_parts(got[c].astype(F32))
        if total is None:
            total, log_w, log_n = state, wide, narrow
        else:
            total = total * fade(wide, narrow) + state
            log_w, log_n = log_w + wide, log_n + narrow
    marks = pieces(log_w, 3) + pieces(log_n, 3) + [jnp.zeros((2, log_w.shape[1]), F32)]
    piece = jnp.concatenate([total] + marks, axis=0).astype(BF16)
    for c in range(count):
        pay[c] = piece


def prefix_kernel(place, got, totals, pay):
    count = got.shape[0]
    mine = place[0]
    total = jnp.zeros((pay.shape[1] - 8, pay.shape[2]), F32)
    for c in range(totals.shape[0]):
        state, wide, narrow = span_parts(totals[c].astype(F32))
        total = jnp.where(c < mine, total * fade(wide, narrow) + state, total)
    pad = jnp.zeros((8, pay.shape[2]), F32)
    for c in range(count):
        pay[c] = jnp.concatenate([total, pad], axis=0).astype(BF16)
        state, wide, narrow = span_parts(got[c].astype(F32))
        total = total * fade(wide, narrow) + state


def apply_kernel(core, base, slope, keys, got, gain, weight, keep, give):
    count = got.shape[0]
    w = STATE_WIDE // count
    n = STATE_NARROW // count
    carried = [got[c].astype(F32) for c in range(count)]
    wide = jnp.concatenate([c[:w] for c in carried], axis=0).astype(BF16)
    narrow = jnp.concatenate([c[w : w + n] for c in carried], axis=0).astype(BF16)
    k = keys[...]
    wide_end = 2 * STATE_WIDE
    from_wide = jnp.dot(k[:, STATE_WIDE:wide_end], wide, preferred_element_type=F32)
    from_narrow = jnp.dot(k[:, wide_end + STATE_NARROW :], narrow, preferred_element_type=F32)
    gated = base[...] + slope[...] * jnp.concatenate([from_wide, from_narrow], axis=1)
    squares = as_row(jnp.sum(gated * gated, axis=1, keepdims=True))
    lanes = squares.shape[1]
    hi_lo = pieces(squares, 2)
    blank = jnp.zeros((2, lanes), F32)
    rest = jnp.zeros((12, lanes), F32)
    marks = jnp.concatenate(hi_lo + [blank, rest], axis=0).astype(BF16)
    given = jnp.concatenate([blank] + hi_lo + [rest], axis=0).astype(BF16)
    scaled = (gated * gain[...]).astype(BF16)
    rows, share = scaled.shape[0], keep.shape[2]
    mine = core[0]
    for target, side, mark in ((give, 1 - mine, given), (keep, mine, marks)):
        for c in range(target.shape[0]):
            at = pl.multiple_of((2 * c + side) * share, share)
            part = jnp.dot(scaled, weight[:, pl.ds(at, share)], preferred_element_type=F32)
            target[c, 0:rows, :] = part.astype(BF16)
            target[c, rows : rows + 16, :] = mark


def merge_kernel(channels, got, residual, gain, lifted_out, tile_out, merged_out):
    rows = residual.shape[1]
    total = got[0].astype(F32)
    for c in range(1, got.shape[0]):
        total = total + got[c].astype(F32)
    squares = jnp.sum(total[rows : rows + 8], axis=0, keepdims=True)
    inverse = as_col(lax.rsqrt(squares / channels + NORM_FLOOR))
    merged = jnp.transpose(residual[...].astype(F32)) + inverse * total[:rows]
    merged = merged.astype(BF16).astype(F32)
    merged_out[...] = jnp.transpose(merged).astype(BF16)
    own = as_row(jnp.sum(merged * merged, axis=1, keepdims=True))
    lifted = (merged * gain[...]).astype(BF16)
    lifted_out[...] = lifted
    edge = lifted[rows - 8 :, :].astype(F32)
    tile = pieces(own, 2) + [jnp.zeros((4, own.shape[1]), F32), edge[6:8]]
    tile_out[...] = jnp.concatenate(tile, axis=0).astype(BF16)


def down_blocks(target, side, down, hidden):
    units = hidden.shape[1]
    share = target.shape[1]
    step = share // (2 * down.shape[1])
    for c in range(target.shape[0]):
        block = down[pl.ds((2 * c + side) * step, step)]
        block = jnp.concatenate([block[:, :, :units], block[:, :, units:]], axis=1)
        part = lax.dot_general(
            block.reshape(share, units), hidden[...], LAST, preferred_element_type=F32
        )
        target[c] = part.astype(BF16)


def keep_kernel(core, hidden, down, keep):
    down_blocks(keep, core[0], down, hidden)


def channel_kernel(
    features, core, own, other, weights, taps, give, hidden, down, lhs, wide, buf, total, sems
):
    chips, high, share = own.shape
    rows = high - 16
    units = hidden.shape[1]
    spans, each, _ = wide.shape
    half = down.shape[1]
    quarters = 4
    copies = []
    for first, last, target, count in ((0, each, wide, quarters), (each, each + half, down, 2)):
        step = spans // count
        for n in range(count):
            part = pl.ds(n * step, step)
            copies.append(
                pltpu.make_async_copy(
                    weights.at[part, first:last], target.at[part], sems.at[len(copies)]
                )
            )
    for copy in copies:
        copy.start()
    mine = core[0]
    marks = jnp.zeros((16, share), F32)
    for c in range(chips):
        first, second = own[c], other[c]
        marks = marks + first[rows:].astype(F32) + second[rows:].astype(F32)
        at = 2 * c * share
        lhs[:, at : at + share] = jnp.where(mine == 0, first, second)
        lhs[:, at + share : at + 2 * share] = jnp.where(mine == 0, second, first)

    def inverse_of(at):
        squares = marks[at : at + 1, :] + marks[at + 1 : at + 2, :]
        return as_col(lax.rsqrt(squares / features + NORM_FLOOR))

    scale, before = inverse_of(0), inverse_of(8)
    step = spans // quarters
    depth = step * each
    for n in range(quarters):
        copies[n].wait()
        block = wide[n * step : (n + 1) * step].reshape(depth, 2 * units)
        part = jnp.dot(
            lhs[:, n * depth : (n + 1) * depth], block, preferred_element_type=F32
        )
        if n == 0:
            total[...] = part
        elif n < quarters - 1:
            total[...] += part
        else:
            part = total[...] + part
            edge = part[rows + 8 :] * before[rows - 8 :, :]
            buf[0:8, :] = edge.astype(BF16).astype(F32)
            buf[8 : 8 + rows, :] = (part[:rows] * scale).astype(BF16).astype(F32)

    def conv(branch):
        first, last = branch * units, (branch + 1) * units
        count = taps.shape[1]
        summed = None
        for k in range(count):
            at = 8 - (count - 1) + k
            term = taps[branch, k : k + 1, :].astype(F32) * buf[at : at + rows, first:last]
            summed = term if summed is None else summed + term
        return summed

    hidden[...] = (silu(conv(0)) * conv(1)).astype(BF16)
    for copy in copies[quarters:]:
        copy.wait()
    down_blocks(give, 1 - mine, down, hidden)


def finish_kernel(merged, got, out):
    total = merged[...].astype(F32)
    for c in range(got.shape[0]):
        total = total + got[c].astype(F32)
    out[...] = total.astype(BF16)


def exchange(parts, axis):
    return lax.all_to_all(parts, axis, split_axis=0, concat_axis=0, tiled=True)


def from_behind(value, axis):
    count = lax.axis_size(axis)
    return lax.ppermute(value, axis, [(source, source + 1) for source in range(count - 1)])


def swapped(value):
    return lax.ppermute(value, "core", [(0, 1), (1, 0)])


def pair_then_chips(kept, given):
    both = (kept.astype(F32) + swapped(given).astype(F32)).astype(BF16)
    return exchange(both, "x")


def local(
    residual,
    values,
    gate_input,
    group_keys,
    time_step,
    decay_rate,
    skip_gain,
    conv_values,
    conv_keys,
    mix_gain,
    out_weight,
    norm_gain,
    hidden_gate,
    hidden_up,
    hidden_conv,
    hidden_down,
):
    rows, cols = values.shape
    key_cols = group_keys.shape[1]
    last = rows // 8 - 1
    whole = lambda a: pl.BlockSpec(a.shape, lambda i: (0, 0))
    own_rows, tail = call(
        pack_kernel,
        [
            ((hidden_gate.shape[0] * 3 // 2, 2 * hidden_gate.shape[1]), BF16),
            ((8, cols + key_cols), BF16),
        ],
        grid=(1,),
        in_specs=[whole(hidden_gate), whole(hidden_up), whole(hidden_gate)]
        + [pl.BlockSpec((8, width), lambda i: (last, 0)) for width in (cols, key_cols)],
        grant=60,
        name="pack",
    )(hidden_gate, hidden_up, hidden_down.T, values, group_keys)
    weights = lax.all_gather(own_rows, SP, axis=0)
    chips = lax.axis_size("x")
    n_tp = chips * lax.axis_size("core")
    n_row = lax.axis_size(SP[1])
    features = residual.shape[0]
    units = hidden_gate.shape[1]
    before = from_behind(tail, SP)
    core = lax.axis_index("core").astype(jnp.int32).reshape(1)
    span = STATE_WIDE // n_row + STATE_NARROW // n_row + 8
    x, keys, run, delta, run_col, pay = call(
        state_kernel,
        [
            ((rows, cols), BF16),
            ((rows, key_cols), BF16),
            ((GROUP_HEADS, rows), F32),
            ((GROUP_HEADS, rows), F32),
            ((rows, GROUP_HEADS), F32),
            ((n_row, span, HALF), BF16),
        ],
        [((rows + 8, cols), F32), ((rows + 8, key_cols), F32)],
        in_specs=[VMEM, VMEM, VMEM, VMEM, SMEM, VMEM, VMEM],
        grant=60,
        name="span_state",
    )(
        values,
        group_keys,
        before,
        time_step,
        decay_rate,
        conv_values,
        conv_keys,
    )
    by_row = exchange(pay, SP[1])
    base, slope = call(
        inside_kernel, [((rows, cols), F32), ((rows, cols), F32)], name="inside_span"
    )(x, keys, run, delta, run_col, jnp.repeat(skip_gain, HEAD_SIZE).reshape(1, -1), gate_input)
    (sums,) = call(
        row_total_kernel, [((lax.axis_size(SP[0]), span, HALF), BF16)], name="row_total"
    )(by_row)
    totals = exchange(sums, SP[0])
    place = lax.axis_index(SP[0]).astype(jnp.int32).reshape(1)
    (starts,) = call(
        prefix_kernel,
        [((n_row, span, HALF), BF16)],
        in_specs=[
            pl.BlockSpec(memory_space=pltpu.SMEM),
            pl.BlockSpec(memory_space=pltpu.VMEM),
            pl.BlockSpec(memory_space=pltpu.VMEM),
        ],
        name="prefix",
    )(place, by_row, totals)
    carried = exchange(starts, SP[1])
    kept, given = call(
        apply_kernel,
        [((chips, rows + 16, features), BF16)] * 2,
        in_specs=[SMEM] + [VMEM] * 6,
        name="apply_project",
    )(core, base, slope, keys, carried, mix_gain.reshape(1, -1), out_weight)
    summed = pair_then_chips(kept, given)
    place_tp = lax.axis_index(("x", "core"))
    own_gain = lax.dynamic_slice_in_dim(norm_gain, place_tp * features, features, 0)
    lifted, tile, merged = call(
        functools.partial(merge_kernel, cols * n_tp),
        [((rows, features), BF16), ((8, features), BF16), ((features, rows), BF16)],
        name="merge",
    )(summed, residual, own_gain.reshape(1, -1))
    stream = jnp.concatenate([lifted, tile, from_behind(tile, SP)], axis=0)
    own_core = exchange(jnp.broadcast_to(stream, (chips, *stream.shape)), "x")
    other_core = swapped(own_core)
    spans, each = weights.shape[0], hidden_gate.shape[0]
    given, hidden, down = call(
        functools.partial(channel_kernel, features * n_tp),
        [
            ((chips, features, rows), BF16),
            ((rows, units), BF16),
            ((spans, each // 2, 2 * units), BF16),
        ],
        [
            ((rows + 16, features * n_tp), BF16),
            ((spans, each, 2 * units), BF16),
            ((rows + 8, 2 * units), F32),
            ((rows + 16, 2 * units), F32),
        ],
        more_scratch=[pltpu.SemaphoreType.DMA((6,))],
        grant=24,
        in_specs=[SMEM, VMEM, VMEM, pl.BlockSpec(memory_space=pltpu.HBM), VMEM],
        out_specs=[VMEM] * 3,
        name="channel_mixer",
    )(
        core, own_core, other_core, pltpu.with_memory_space_constraint(weights, pltpu.HBM), hidden_conv
    )
    (kept,) = call(
        keep_kernel,
        [((chips, features, rows), BF16)],
        in_specs=[SMEM, VMEM, VMEM],
        out_specs=[VMEM],
        name="keep_blocks",
    )(core, hidden, down)
    got = pair_then_chips(kept, given)
    (out,) = call(finish_kernel, [((features, rows), BF16)], name="finish")(merged, got)
    return out


def solution(mesh):
    split = Mesh(mesh.devices.reshape(8, 8, 4, 2), ("sp_0", "sp_1", "x", "core"))
    tp = ("x", "core")
    placed = (
        P(tp, SP),
        P(SP, tp),
        P(SP, tp),
        P(SP, tp),
        P(tp, SP),
        P(tp),
        P(tp),
        P(None, tp),
        P(None, tp),
        P(tp),
        P(tp, None),
        P(),
        P(SP, tp),
        P(SP, tp),
        P(None, None, tp),
        P(tp, SP),
    )
    return jax.shard_map(local, mesh=split, in_specs=placed, out_specs=P(tp, SP), check_vma=False)
```

```python
import functools

import jax
import jax.numpy as jnp
from jax import lax
from jax.experimental import pallas as pl
from jax.experimental.pallas import tpu as pltpu
from jax.sharding import Mesh
from jax.sharding import PartitionSpec as P

GROUP_HEADS = 8
HEAD_SIZE = 64
STATE_WIDE = 128
STATE_NARROW = 64
HALF = GROUP_HEADS // 2 * HEAD_SIZE
SP = ("sp_0", "sp_1")
NORM_FLOOR = 0.1
F32 = jnp.float32
BF16 = jnp.bfloat16
HIGHEST = lax.Precision.HIGHEST
LAST = (((1,), (1,)), ((), ()))
FIRST = (((0,), (0,)), ((), ()))


SMEM = pl.BlockSpec(memory_space=pltpu.SMEM)
VMEM = pl.BlockSpec(memory_space=pltpu.VMEM)


def call(kernel, outs, scratch=(), grant=12, more_scratch=(), **more):
    return pl.pallas_call(
        kernel,
        out_shape=[jax.ShapeDtypeStruct(shape, kind) for shape, kind in outs],
        scratch_shapes=[pltpu.VMEM(shape, kind) for shape, kind in scratch] + list(more_scratch),
        compiler_params=pltpu.CompilerParams(vmem_limit_bytes=grant << 20),
        **more,
    )


def pack_kernel(gate, up, down, values, keys, rows_out, tail_out):
    rows, units = gate.shape
    cols = values.shape[1]
    rows_out[:rows, :units] = gate[...]
    rows_out[:rows, units:] = up[...]
    rows_out[rows:, :units] = down[: rows // 2]
    rows_out[rows:, units:] = down[rows // 2 :]
    tail_out[:, :cols] = values[...]
    tail_out[:, cols:] = keys[...]


def silu(a):
    return a / (1.0 + jnp.exp(-a))


def pieces(row, count):
    found = []
    for _ in range(count):
        part = row.astype(BF16).astype(F32)
        found.append(part)
        row = row - part
    return found


def head_lanes(cols):
    rows = cols.shape[0]
    lane = lax.broadcasted_iota(jnp.int32, (rows, 2 * HEAD_SIZE), 1)
    both = [
        jnp.where(lane < HEAD_SIZE, cols[:, h : h + 1], cols[:, h + 1 : h + 2])
        for h in range(0, GROUP_HEADS, 2)
    ]
    return jnp.concatenate(both, axis=1)


def as_row(col):
    return jnp.transpose(jnp.broadcast_to(col, (col.shape[0], 128)))[0:1, :]


def as_col(row):
    return jnp.transpose(jnp.broadcast_to(row, (8, row.shape[1])))[:, 0:1]


def conv_silu(buf, taps, rows):
    count = taps.shape[0]
    total = taps[count - 1 : count, :].astype(F32) * buf[8 : 8 + rows, :]
    for k in range(count - 1):
        at = 8 - (count - 1) + k
        total = total + taps[k : k + 1, :].astype(F32) * buf[at : at + rows, :]
    return silu(total)


def state_kernel(
    values, keys, before, step, rate, taps_v, taps_k, x_out, key_out, run_out, delta_out, run_col, pay, vbuf, kbuf
):
    rows, cols = values.shape
    vbuf[0:8, :] = before[:, :cols].astype(F32)
    vbuf[8 : 8 + rows, :] = values[...].astype(F32)
    kbuf[0:8, :] = before[:, cols:].astype(F32)
    kbuf[8 : 8 + rows, :] = keys[...].astype(F32)
    x = conv_silu(vbuf, taps_v, rows)
    k = conv_silu(kbuf, taps_k, rows).astype(BF16)
    x_out[...] = x.astype(BF16)
    key_out[...] = k
    pre = step[...]
    delta = jnp.maximum(pre, 0.0) + jnp.log1p(jnp.exp(-jnp.abs(pre)))
    upper = lax.broadcasted_iota(jnp.int32, (rows, rows), 0) <= lax.broadcasted_iota(
        jnp.int32, (rows, rows), 1
    )
    head = lax.broadcasted_iota(jnp.int32, delta.shape, 0)
    rates = jnp.zeros(delta.shape, F32)
    for h in range(GROUP_HEADS):
        rates = jnp.where(head == h, rate[h], rates)
    run = jnp.dot(-rates * delta, upper.astype(F32), precision=HIGHEST, preferred_element_type=F32)
    run_out[...] = run
    delta_out[...] = delta
    run_t = jnp.transpose(run)
    run_col[...] = run_t
    end = run_t[rows - 1 : rows, :]
    to_end = jnp.exp(end - run_t) * jnp.transpose(delta)
    weighted = (x * head_lanes(to_end)).astype(BF16)
    wide = lax.dot_general(k[:, :STATE_WIDE], weighted[:, :HALF], FIRST, preferred_element_type=F32)
    narrow = lax.dot_general(
        k[:, 2 * STATE_WIDE :], weighted[:, HALF:], FIRST, preferred_element_type=F32
    )
    ends = head_lanes(jnp.broadcast_to(end, (8, GROUP_HEADS)))[0:1, :]
    marks = pieces(ends[:, :HALF], 3) + pieces(ends[:, HALF:], 3) + [jnp.zeros((2, HALF), F32)]
    count = pay.shape[0]
    w, n = STATE_WIDE // count, STATE_NARROW // count
    for c in range(count):
        part = [wide[c * w : (c + 1) * w], narrow[c * n : (c + 1) * n]] + marks
        pay[c] = jnp.concatenate(part, axis=0).astype(BF16)


def inside_kernel(x, keys, run, delta, run_col, skip, gate, base_out, slope_out):
    rows = x.shape[0]
    xs = x[...]
    k = keys[...]
    wide_end = 2 * STATE_WIDE
    score_w = lax.dot_general(k[:, STATE_WIDE:wide_end], k[:, :STATE_WIDE], LAST, preferred_element_type=F32)
    score_n = lax.dot_general(
        k[:, wide_end + STATE_NARROW :], k[:, wide_end : wide_end + STATE_NARROW], LAST, preferred_element_type=F32
    )
    keep = lax.broadcasted_iota(jnp.int32, (rows, rows), 0) >= lax.broadcasted_iota(
        jnp.int32, (rows, rows), 1
    )
    runs, deltas, cols = run[...], delta[...], run_col[...]
    outs = []
    for h in range(GROUP_HEADS):
        gap = jnp.where(keep, cols[:, h : h + 1] - runs[h : h + 1, :], -jnp.inf)
        score = score_w if h < GROUP_HEADS // 2 else score_n
        mixed = (score * (jnp.exp(gap) * deltas[h : h + 1, :])).astype(BF16)
        outs.append(
            jnp.dot(mixed, xs[:, h * HEAD_SIZE : (h + 1) * HEAD_SIZE], preferred_element_type=F32)
        )
    opened = silu(gate[...].astype(F32))
    direct = jnp.concatenate(outs, axis=1) + skip[...] * xs.astype(F32)
    base_out[...] = direct * opened
    slope_out[...] = head_lanes(jnp.exp(cols)) * opened


def span_parts(piece):
    w = STATE_WIDE // 8
    n = STATE_NARROW // 8
    state = piece[: w + n]
    at = w + n
    wide = piece[at : at + 1] + piece[at + 1 : at + 2] + piece[at + 2 : at + 3]
    narrow = piece[at + 3 : at + 4] + piece[at + 4 : at + 5] + piece[at + 5 : at + 6]
    return state, wide, narrow


def fade(wide, narrow):
    w = STATE_WIDE // 8
    n = STATE_NARROW // 8
    lanes = wide.shape[1]
    return jnp.concatenate(
        [
            jnp.broadcast_to(jnp.exp(wide), (w, lanes)),
            jnp.broadcast_to(jnp.exp(narrow), (n, lanes)),
        ],
        axis=0,
    )


def row_total_kernel(got, pay):
    count = got.shape[0]
    total = None
    for c in range(count):
        state, wide, narrow = span_parts(got[c].astype(F32))
        if total is None:
            total, log_w, log_n = state, wide, narrow
        else:
            total = total * fade(wide, narrow) + state
            log_w, log_n = log_w + wide, log_n + narrow
    marks = pieces(log_w, 3) + pieces(log_n, 3) + [jnp.zeros((2, log_w.shape[1]), F32)]
    piece = jnp.concatenate([total] + marks, axis=0).astype(BF16)
    for c in range(count):
        pay[c] = piece


def prefix_kernel(place, got, totals, pay):
    count = got.shape[0]
    mine = place[0]
    total = jnp.zeros((pay.shape[1] - 8, pay.shape[2]), F32)
    for c in range(totals.shape[0]):
        state, wide, narrow = span_parts(totals[c].astype(F32))
        total = jnp.where(c < mine, total * fade(wide, narrow) + state, total)
    pad = jnp.zeros((8, pay.shape[2]), F32)
    for c in range(count):
        pay[c] = jnp.concatenate([total, pad], axis=0).astype(BF16)
        state, wide, narrow = span_parts(got[c].astype(F32))
        total = total * fade(wide, narrow) + state


def apply_kernel(core, base, slope, keys, got, gain, weight, keep, give):
    count = got.shape[0]
    w = STATE_WIDE // count
    n = STATE_NARROW // count
    carried = [got[c].astype(F32) for c in range(count)]
    wide = jnp.concatenate([c[:w] for c in carried], axis=0).astype(BF16)
    narrow = jnp.concatenate([c[w : w + n] for c in carried], axis=0).astype(BF16)
    k = keys[...]
    wide_end = 2 * STATE_WIDE
    from_wide = jnp.dot(k[:, STATE_WIDE:wide_end], wide, preferred_element_type=F32)
    from_narrow = jnp.dot(k[:, wide_end + STATE_NARROW :], narrow, preferred_element_type=F32)
    gated = base[...] + slope[...] * jnp.concatenate([from_wide, from_narrow], axis=1)
    squares = as_row(jnp.sum(gated * gated, axis=1, keepdims=True))
    lanes = squares.shape[1]
    hi_lo = pieces(squares, 2)
    blank = jnp.zeros((2, lanes), F32)
    rest = jnp.zeros((12, lanes), F32)
    marks = jnp.concatenate(hi_lo + [blank, rest], axis=0).astype(BF16)
    given = jnp.concatenate([blank] + hi_lo + [rest], axis=0).astype(BF16)
    scaled = (gated * gain[...]).astype(BF16)
    rows, share = scaled.shape[0], keep.shape[2]
    mine = core[0]
    for target, side, mark in ((give, 1 - mine, given), (keep, mine, marks)):
        for c in range(target.shape[0]):
            at = pl.multiple_of((2 * c + side) * share, share)
            part = jnp.dot(scaled, weight[:, pl.ds(at, share)], preferred_element_type=F32)
            target[c, 0:rows, :] = part.astype(BF16)
            target[c, rows : rows + 16, :] = mark


def merge_kernel(channels, got, residual, gain, lifted_out, tile_out, merged_out):
    rows = residual.shape[1]
    total = got[0].astype(F32)
    for c in range(1, got.shape[0]):
        total = total + got[c].astype(F32)
    squares = jnp.sum(total[rows : rows + 8], axis=0, keepdims=True)
    inverse = as_col(lax.rsqrt(squares / channels + NORM_FLOOR))
    merged = jnp.transpose(residual[...].astype(F32)) + inverse * total[:rows]
    merged = merged.astype(BF16).astype(F32)
    merged_out[...] = jnp.transpose(merged).astype(BF16)
    own = as_row(jnp.sum(merged * merged, axis=1, keepdims=True))
    lifted = (merged * gain[...]).astype(BF16)
    lifted_out[...] = lifted
    edge = lifted[rows - 8 :, :].astype(F32)
    tile = pieces(own, 2) + [jnp.zeros((4, own.shape[1]), F32), edge[6:8]]
    tile_out[...] = jnp.concatenate(tile, axis=0).astype(BF16)


def down_blocks(target, side, down, hidden):
    units = hidden.shape[1]
    share = target.shape[1]
    step = share // (2 * down.shape[1])
    for c in range(target.shape[0]):
        block = down[pl.ds((2 * c + side) * step, step)]
        block = jnp.concatenate([block[:, :, :units], block[:, :, units:]], axis=1)
        part = lax.dot_general(
            block.reshape(share, units), hidden[...], LAST, preferred_element_type=F32
        )
        target[c] = part.astype(BF16)


def keep_kernel(core, hidden, down, keep):
    down_blocks(keep, core[0], down, hidden)


def channel_kernel(
    features, core, own, other, weights, taps, give, hidden, down, lhs, wide, total, sems
):
    chips, high, share = own.shape
    rows = high - 16
    units = hidden.shape[1]
    spans, each, _ = wide.shape
    half = down.shape[1]
    quarters = 4
    copies = []
    for first, last, target, count in ((0, each, wide, quarters), (each, each + half, down, 2)):
        step = spans // count
        for n in range(count):
            part = pl.ds(n * step, step)
            copies.append(
                pltpu.make_async_copy(
                    weights.at[part, first:last], target.at[part], sems.at[len(copies)]
                )
            )
    for copy in copies:
        copy.start()
    mine = core[0]
    marks = jnp.zeros((16, share), F32)
    for c in range(chips):
        first, second = own[c], other[c]
        marks = marks + first[rows:].astype(F32) + second[rows:].astype(F32)
        at = 2 * c * share
        lhs[:, at : at + share] = jnp.where(mine == 0, first, second)
        lhs[:, at + share : at + 2 * share] = jnp.where(mine == 0, second, first)

    def inverse_of(at):
        squares = marks[at : at + 1, :] + marks[at + 1 : at + 2, :]
        return as_col(lax.rsqrt(squares / features + NORM_FLOOR))

    scale = jnp.concatenate([inverse_of(0), inverse_of(8)[rows - 16 :]], axis=0)
    step = spans // quarters
    depth = step * each
    for n in range(quarters):
        copies[n].wait()
        block = wide[n * step : (n + 1) * step].reshape(depth, 2 * units)
        part = jnp.dot(
            lhs[:, n * depth : (n + 1) * depth], block, preferred_element_type=F32
        )
        if n == 0:
            total[...] = part
        elif n < quarters - 1:
            total[...] += part
        else:
            part = (total[...] + part) * scale
            total[...] = part.astype(BF16).astype(F32)

    def conv(branch, lane):
        at = branch * units + lane
        held = total[:, at : at + 128]
        row = taps[branch, :, lane : lane + 128].astype(F32)
        count = row.shape[0]
        summed = row[count - 1 : count] * held
        for k in range(1, count):
            summed = summed + row[count - 1 - k : count - k] * pltpu.roll(held, k, 0)
        return summed[:rows]

    for lane in range(0, units, 128):
        gated = silu(conv(0, lane)) * conv(1, lane)
        hidden[:, lane : lane + 128] = gated.astype(BF16)
    for copy in copies[quarters:]:
        copy.wait()
    down_blocks(give, 1 - mine, down, hidden)


def finish_kernel(merged, got, out):
    total = merged[...].astype(F32)
    for c in range(got.shape[0]):
        total = total + got[c].astype(F32)
    out[...] = total.astype(BF16)


def exchange(parts, axis):
    return lax.all_to_all(parts, axis, split_axis=0, concat_axis=0, tiled=True)


def from_behind(value, axis):
    count = lax.axis_size(axis)
    return lax.ppermute(value, axis, [(source, source + 1) for source in range(count - 1)])


def swapped(value):
    return lax.ppermute(value, "core", [(0, 1), (1, 0)])


def pair_then_chips(kept, given):
    both = (kept.astype(F32) + swapped(given).astype(F32)).astype(BF16)
    return exchange(both, "x")


def local(
    residual,
    values,
    gate_input,
    group_keys,
    time_step,
    decay_rate,
    skip_gain,
    conv_values,
    conv_keys,
    mix_gain,
    out_weight,
    norm_gain,
    hidden_gate,
    hidden_up,
    hidden_conv,
    hidden_down,
):
    rows, cols = values.shape
    key_cols = group_keys.shape[1]
    last = rows // 8 - 1
    whole = lambda a: pl.BlockSpec(a.shape, lambda i: (0, 0))
    own_rows, tail = call(
        pack_kernel,
        [
            ((hidden_gate.shape[0] * 3 // 2, 2 * hidden_gate.shape[1]), BF16),
            ((8, cols + key_cols), BF16),
        ],
        grid=(1,),
        in_specs=[whole(hidden_gate), whole(hidden_up), whole(hidden_gate)]
        + [pl.BlockSpec((8, width), lambda i: (last, 0)) for width in (cols, key_cols)],
        grant=60,
        name="pack",
    )(hidden_gate, hidden_up, hidden_down.T, values, group_keys)
    weights = lax.all_gather(own_rows, SP, axis=0)
    chips = lax.axis_size("x")
    n_tp = chips * lax.axis_size("core")
    n_row = lax.axis_size(SP[1])
    features = residual.shape[0]
    units = hidden_gate.shape[1]
    before = from_behind(tail, SP)
    core = lax.axis_index("core").astype(jnp.int32).reshape(1)
    span = STATE_WIDE // n_row + STATE_NARROW // n_row + 8
    x, keys, run, delta, run_col, pay = call(
        state_kernel,
        [
            ((rows, cols), BF16),
            ((rows, key_cols), BF16),
            ((GROUP_HEADS, rows), F32),
            ((GROUP_HEADS, rows), F32),
            ((rows, GROUP_HEADS), F32),
            ((n_row, span, HALF), BF16),
        ],
        [((rows + 8, cols), F32), ((rows + 8, key_cols), F32)],
        in_specs=[VMEM, VMEM, VMEM, VMEM, SMEM, VMEM, VMEM],
        grant=60,
        name="span_state",
    )(
        values,
        group_keys,
        before,
        time_step,
        decay_rate,
        conv_values,
        conv_keys,
    )
    by_row = exchange(pay, SP[1])
    base, slope = call(
        inside_kernel, [((rows, cols), F32), ((rows, cols), F32)], name="inside_span"
    )(x, keys, run, delta, run_col, jnp.repeat(skip_gain, HEAD_SIZE).reshape(1, -1), gate_input)
    (sums,) = call(
        row_total_kernel, [((lax.axis_size(SP[0]), span, HALF), BF16)], name="row_total"
    )(by_row)
    totals = exchange(sums, SP[0])
    place = lax.axis_index(SP[0]).astype(jnp.int32).reshape(1)
    (starts,) = call(
        prefix_kernel,
        [((n_row, span, HALF), BF16)],
        in_specs=[
            pl.BlockSpec(memory_space=pltpu.SMEM),
            pl.BlockSpec(memory_space=pltpu.VMEM),
            pl.BlockSpec(memory_space=pltpu.VMEM),
        ],
        name="prefix",
    )(place, by_row, totals)
    carried = exchange(starts, SP[1])
    kept, given = call(
        apply_kernel,
        [((chips, rows + 16, features), BF16)] * 2,
        in_specs=[SMEM] + [VMEM] * 6,
        name="apply_project",
    )(core, base, slope, keys, carried, mix_gain.reshape(1, -1), out_weight)
    summed = pair_then_chips(kept, given)
    place_tp = lax.axis_index(("x", "core"))
    own_gain = lax.dynamic_slice_in_dim(norm_gain, place_tp * features, features, 0)
    lifted, tile, merged = call(
        functools.partial(merge_kernel, cols * n_tp),
        [((rows, features), BF16), ((8, features), BF16), ((features, rows), BF16)],
        name="merge",
    )(summed, residual, own_gain.reshape(1, -1))
    stream = jnp.concatenate([lifted, tile, from_behind(tile, SP)], axis=0)
    own_core = exchange(jnp.broadcast_to(stream, (chips, *stream.shape)), "x")
    other_core = swapped(own_core)
    spans, each = weights.shape[0], hidden_gate.shape[0]
    given, hidden, down = call(
        functools.partial(channel_kernel, features * n_tp),
        [
            ((chips, features, rows), BF16),
            ((rows, units), BF16),
            ((spans, each // 2, 2 * units), BF16),
        ],
        [
            ((rows + 16, features * n_tp), BF16),
            ((spans, each, 2 * units), BF16),
            ((rows + 16, 2 * units), F32),
        ],
        more_scratch=[pltpu.SemaphoreType.DMA((6,))],
        grant=24,
        in_specs=[SMEM, VMEM, VMEM, pl.BlockSpec(memory_space=pltpu.HBM), VMEM],
        out_specs=[VMEM] * 3,
        name="channel_mixer",
    )(
        core, own_core, other_core, pltpu.with_memory_space_constraint(weights, pltpu.HBM), hidden_conv
    )
    (kept,) = call(
        keep_kernel,
        [((chips, features, rows), BF16)],
        in_specs=[SMEM, VMEM, VMEM],
        out_specs=[VMEM],
        name="keep_blocks",
    )(core, hidden, down)
    got = pair_then_chips(kept, given)
    (out,) = call(finish_kernel, [((features, rows), BF16)], name="finish")(merged, got)
    return out


def solution(mesh):
    split = Mesh(mesh.devices.reshape(8, 8, 4, 2), ("sp_0", "sp_1", "x", "core"))
    tp = ("x", "core")
    placed = (
        P(tp, SP),
        P(SP, tp),
        P(SP, tp),
        P(SP, tp),
        P(tp, SP),
        P(tp),
        P(tp),
        P(None, tp),
        P(None, tp),
        P(tp),
        P(tp, None),
        P(),
        P(SP, tp),
        P(SP, tp),
        P(None, None, tp),
        P(tp, SP),
    )
    return jax.shard_map(local, mesh=split, in_specs=placed, out_specs=P(tp, SP), check_vma=False)
```

```python
import functools

import jax
import jax.numpy as jnp
from jax import lax
from jax.experimental import pallas as pl
from jax.experimental.pallas import tpu as pltpu
from jax.sharding import Mesh
from jax.sharding import PartitionSpec as P

GROUP_HEADS = 8
HEAD_SIZE = 64
STATE_WIDE = 128
STATE_NARROW = 64
HALF = GROUP_HEADS // 2 * HEAD_SIZE
SP = ("sp_0", "sp_1")
NORM_FLOOR = 0.1
F32 = jnp.float32
BF16 = jnp.bfloat16
HIGHEST = lax.Precision.HIGHEST
LAST = (((1,), (1,)), ((), ()))
FIRST = (((0,), (0,)), ((), ()))


SMEM = pl.BlockSpec(memory_space=pltpu.SMEM)
VMEM = pl.BlockSpec(memory_space=pltpu.VMEM)


def call(kernel, outs, scratch=(), grant=12, more_scratch=(), **more):
    return pl.pallas_call(
        kernel,
        out_shape=[jax.ShapeDtypeStruct(shape, kind) for shape, kind in outs],
        scratch_shapes=[pltpu.VMEM(shape, kind) for shape, kind in scratch] + list(more_scratch),
        compiler_params=pltpu.CompilerParams(vmem_limit_bytes=grant << 20),
        **more,
    )


def pack_kernel(gate, up, down, values, keys, rows_out, tail_out):
    rows, units = gate.shape
    cols = values.shape[1]
    rows_out[:rows, :units] = gate[...]
    rows_out[:rows, units:] = up[...]
    rows_out[rows:, :units] = down[: rows // 2]
    rows_out[rows:, units:] = down[rows // 2 :]
    tail_out[:, :cols] = values[...]
    tail_out[:, cols:] = keys[...]


def silu(a):
    return a / (1.0 + jnp.exp(-a))


def pieces(row, count):
    found = []
    for _ in range(count):
        part = row.astype(BF16).astype(F32)
        found.append(part)
        row = row - part
    return found


def head_lanes(cols):
    rows = cols.shape[0]
    lane = lax.broadcasted_iota(jnp.int32, (rows, 2 * HEAD_SIZE), 1)
    both = [
        jnp.where(lane < HEAD_SIZE, cols[:, h : h + 1], cols[:, h + 1 : h + 2])
        for h in range(0, GROUP_HEADS, 2)
    ]
    return jnp.concatenate(both, axis=1)


def as_row(col):
    return jnp.transpose(jnp.broadcast_to(col, (col.shape[0], 128)))[0:1, :]


def as_col(row):
    return jnp.transpose(jnp.broadcast_to(row, (8, row.shape[1])))[:, 0:1]


def conv_silu(buf, taps, rows):
    count = taps.shape[0]
    total = taps[count - 1 : count, :].astype(F32) * buf[8 : 8 + rows, :]
    for k in range(count - 1):
        at = 8 - (count - 1) + k
        total = total + taps[k : k + 1, :].astype(F32) * buf[at : at + rows, :]
    return silu(total)


def state_kernel(
    values, keys, before, step, rate, taps_v, taps_k, x_out, key_out, run_out, delta_out, run_col, pay, vbuf, kbuf
):
    rows, cols = values.shape
    vbuf[0:8, :] = before[:, :cols].astype(F32)
    vbuf[8 : 8 + rows, :] = values[...].astype(F32)
    kbuf[0:8, :] = before[:, cols:].astype(F32)
    kbuf[8 : 8 + rows, :] = keys[...].astype(F32)
    x = conv_silu(vbuf, taps_v, rows)
    k = conv_silu(kbuf, taps_k, rows).astype(BF16)
    x_out[...] = x.astype(BF16)
    key_out[...] = k
    pre = step[...]
    delta = jnp.maximum(pre, 0.0) + jnp.log1p(jnp.exp(-jnp.abs(pre)))
    upper = lax.broadcasted_iota(jnp.int32, (rows, rows), 0) <= lax.broadcasted_iota(
        jnp.int32, (rows, rows), 1
    )
    head = lax.broadcasted_iota(jnp.int32, delta.shape, 0)
    rates = jnp.zeros(delta.shape, F32)
    for h in range(GROUP_HEADS):
        rates = jnp.where(head == h, rate[h], rates)
    run = jnp.dot(-rates * delta, upper.astype(F32), precision=HIGHEST, preferred_element_type=F32)
    run_out[...] = run
    delta_out[...] = delta
    run_t = jnp.transpose(run)
    run_col[...] = run_t
    end = run_t[rows - 1 : rows, :]
    to_end = jnp.exp(end - run_t) * jnp.transpose(delta)
    weighted = (x * head_lanes(to_end)).astype(BF16)
    wide = lax.dot_general(k[:, :STATE_WIDE], weighted[:, :HALF], FIRST, preferred_element_type=F32)
    narrow = lax.dot_general(
        k[:, 2 * STATE_WIDE :], weighted[:, HALF:], FIRST, preferred_element_type=F32
    )
    ends = head_lanes(jnp.broadcast_to(end, (8, GROUP_HEADS)))[0:1, :]
    marks = pieces(ends[:, :HALF], 3) + pieces(ends[:, HALF:], 3) + [jnp.zeros((2, HALF), F32)]
    count = pay.shape[0]
    w, n = STATE_WIDE // count, STATE_NARROW // count
    for c in range(count):
        part = [wide[c * w : (c + 1) * w], narrow[c * n : (c + 1) * n]] + marks
        pay[c] = jnp.concatenate(part, axis=0).astype(BF16)


def inside_kernel(x, keys, run, delta, run_col, skip, gate, base_out, slope_out):
    rows = x.shape[0]
    xs = x[...]
    k = keys[...]
    wide_end = 2 * STATE_WIDE
    score_w = lax.dot_general(k[:, STATE_WIDE:wide_end], k[:, :STATE_WIDE], LAST, preferred_element_type=F32)
    score_n = lax.dot_general(
        k[:, wide_end + STATE_NARROW :], k[:, wide_end : wide_end + STATE_NARROW], LAST, preferred_element_type=F32
    )
    keep = lax.broadcasted_iota(jnp.int32, (rows, rows), 0) >= lax.broadcasted_iota(
        jnp.int32, (rows, rows), 1
    )
    runs, deltas, cols = run[...], delta[...], run_col[...]
    outs = []
    for h in range(GROUP_HEADS):
        gap = jnp.where(keep, cols[:, h : h + 1] - runs[h : h + 1, :], -jnp.inf)
        score = score_w if h < GROUP_HEADS // 2 else score_n
        mixed = (score * (jnp.exp(gap) * deltas[h : h + 1, :])).astype(BF16)
        outs.append(
            jnp.dot(mixed, xs[:, h * HEAD_SIZE : (h + 1) * HEAD_SIZE], preferred_element_type=F32)
        )
    opened = silu(gate[...].astype(F32))
    direct = jnp.concatenate(outs, axis=1) + skip[...] * xs.astype(F32)
    base_out[...] = direct * opened
    slope_out[...] = head_lanes(jnp.exp(cols)) * opened


def span_parts(piece):
    w = STATE_WIDE // 8
    n = STATE_NARROW // 8
    state = piece[: w + n]
    at = w + n
    wide = piece[at : at + 1] + piece[at + 1 : at + 2] + piece[at + 2 : at + 3]
    narrow = piece[at + 3 : at + 4] + piece[at + 4 : at + 5] + piece[at + 5 : at + 6]
    return state, wide, narrow


def fade(wide, narrow):
    w = STATE_WIDE // 8
    n = STATE_NARROW // 8
    lanes = wide.shape[1]
    return jnp.concatenate(
        [
            jnp.broadcast_to(jnp.exp(wide), (w, lanes)),
            jnp.broadcast_to(jnp.exp(narrow), (n, lanes)),
        ],
        axis=0,
    )


def row_total_kernel(got, pay):
    count = got.shape[0]
    total = None
    for c in range(count):
        state, wide, narrow = span_parts(got[c].astype(F32))
        if total is None:
            total, log_w, log_n = state, wide, narrow
        else:
            total = total * fade(wide, narrow) + state
            log_w, log_n = log_w + wide, log_n + narrow
    marks = pieces(log_w, 3) + pieces(log_n, 3) + [jnp.zeros((2, log_w.shape[1]), F32)]
    piece = jnp.concatenate([total] + marks, axis=0).astype(BF16)
    for c in range(count):
        pay[c] = piece


def prefix_kernel(place, got, totals, pay):
    count = got.shape[0]
    mine = place[0]
    total = jnp.zeros((pay.shape[1], pay.shape[2]), F32)
    for c in range(totals.shape[0]):
        state, wide, narrow = span_parts(totals[c].astype(F32))
        total = jnp.where(c < mine, total * fade(wide, narrow) + state, total)
    for c in range(count):
        pay[c] = total.astype(BF16)
        state, wide, narrow = span_parts(got[c].astype(F32))
        total = total * fade(wide, narrow) + state


def apply_kernel(core, base, slope, keys, got, gain, weight, keep, give):
    count = got.shape[0]
    w = STATE_WIDE // count
    n = STATE_NARROW // count
    carried = [got[c].astype(F32) for c in range(count)]
    wide = jnp.concatenate([c[:w] for c in carried], axis=0).astype(BF16)
    narrow = jnp.concatenate([c[w : w + n] for c in carried], axis=0).astype(BF16)
    k = keys[...]
    wide_end = 2 * STATE_WIDE
    from_wide = jnp.dot(k[:, STATE_WIDE:wide_end], wide, preferred_element_type=F32)
    from_narrow = jnp.dot(k[:, wide_end + STATE_NARROW :], narrow, preferred_element_type=F32)
    gated = base[...] + slope[...] * jnp.concatenate([from_wide, from_narrow], axis=1)
    squares = as_row(jnp.sum(gated * gated, axis=1, keepdims=True))
    lanes = squares.shape[1]
    hi_lo = pieces(squares, 2)
    blank = jnp.zeros((2, lanes), F32)
    rest = jnp.zeros((12, lanes), F32)
    marks = jnp.concatenate(hi_lo + [blank, rest], axis=0).astype(BF16)
    given = jnp.concatenate([blank] + hi_lo + [rest], axis=0).astype(BF16)
    scaled = (gated * gain[...]).astype(BF16)
    rows, share = scaled.shape[0], keep.shape[2]
    mine = core[0]
    for target, side, mark in ((give, 1 - mine, given), (keep, mine, marks)):
        for c in range(target.shape[0]):
            at = pl.multiple_of((2 * c + side) * share, share)
            part = jnp.dot(scaled, weight[:, pl.ds(at, share)], preferred_element_type=F32)
            target[c, 0:rows, :] = part.astype(BF16)
            target[c, rows : rows + 16, :] = mark


def merge_kernel(channels, got, residual, gain, lifted_out, tile_out, merged_out):
    rows = residual.shape[1]
    total = got[0].astype(F32)
    for c in range(1, got.shape[0]):
        total = total + got[c].astype(F32)
    squares = jnp.sum(total[rows : rows + 8], axis=0, keepdims=True)
    inverse = as_col(lax.rsqrt(squares / channels + NORM_FLOOR))
    merged = jnp.transpose(residual[...].astype(F32)) + inverse * total[:rows]
    merged = merged.astype(BF16).astype(F32)
    merged_out[...] = jnp.transpose(merged).astype(BF16)
    own = as_row(jnp.sum(merged * merged, axis=1, keepdims=True))
    lifted = (merged * gain[...]).astype(BF16)
    lifted_out[...] = lifted
    edge = lifted[rows - 8 :, :].astype(F32)
    tile = pieces(own, 2) + [jnp.zeros((4, own.shape[1]), F32), edge[6:8]]
    tile_out[...] = jnp.concatenate(tile, axis=0).astype(BF16)


def down_blocks(target, side, down, hidden):
    units = hidden.shape[1]
    share = target.shape[1]
    step = share // (2 * down.shape[1])
    for c in range(target.shape[0]):
        block = down[pl.ds((2 * c + side) * step, step)]
        block = jnp.concatenate([block[:, :, :units], block[:, :, units:]], axis=1)
        part = lax.dot_general(
            block.reshape(share, units), hidden[...], LAST, preferred_element_type=F32
        )
        target[c] = part.astype(BF16)


def keep_kernel(core, hidden, down, keep):
    down_blocks(keep, core[0], down, hidden)


def channel_kernel(
    features, core, own, other, weights, taps, give, hidden, down, lhs, wide, buf, total, sems
):
    chips, high, share = own.shape
    rows = high - 16
    units = hidden.shape[1]
    spans, each, _ = wide.shape
    half = down.shape[1]
    quarters = 4
    copies = []
    for first, last, target, count in ((0, each, wide, quarters), (each, each + half, down, 2)):
        step = spans // count
        for n in range(count):
            part = pl.ds(n * step, step)
            copies.append(
                pltpu.make_async_copy(
                    weights.at[part, first:last], target.at[part], sems.at[len(copies)]
                )
            )
    for copy in copies:
        copy.start()
    mine = core[0]
    marks = jnp.zeros((16, share), F32)
    for c in range(chips):
        first, second = own[c], other[c]
        marks = marks + first[rows:].astype(F32) + second[rows:].astype(F32)
        at = 2 * c * share
        lhs[:, at : at + share] = jnp.where(mine == 0, first, second)
        lhs[:, at + share : at + 2 * share] = jnp.where(mine == 0, second, first)

    def inverse_of(at):
        squares = marks[at : at + 1, :] + marks[at + 1 : at + 2, :]
        return as_col(lax.rsqrt(squares / features + NORM_FLOOR))

    scale, before = inverse_of(0), inverse_of(8)
    step = spans // quarters
    depth = step * each
    for n in range(quarters):
        copies[n].wait()
        block = wide[n * step : (n + 1) * step].reshape(depth, 2 * units)
        part = jnp.dot(
            lhs[:, n * depth : (n + 1) * depth], block, preferred_element_type=F32
        )
        if n == 0:
            total[...] = part
        elif n < quarters - 1:
            total[...] += part
        else:
            part = total[...] + part
            edge = part[rows + 8 :] * before[rows - 8 :, :]
            buf[0:8, :] = edge.astype(BF16).astype(F32)
            buf[8 : 8 + rows, :] = (part[:rows] * scale).astype(BF16).astype(F32)

    def conv(branch):
        first, last = branch * units, (branch + 1) * units
        count = taps.shape[1]
        summed = None
        for k in range(count):
            at = 8 - (count - 1) + k
            term = taps[branch, k : k + 1, :].astype(F32) * buf[at : at + rows, first:last]
            summed = term if summed is None else summed + term
        return summed

    hidden[...] = (silu(conv(0)) * conv(1)).astype(BF16)
    for copy in copies[quarters:]:
        copy.wait()
    down_blocks(give, 1 - mine, down, hidden)


def finish_kernel(merged, got, out):
    total = merged[...].astype(F32)
    for c in range(got.shape[0]):
        total = total + got[c].astype(F32)
    out[...] = total.astype(BF16)


def exchange(parts, axis):
    return lax.all_to_all(parts, axis, split_axis=0, concat_axis=0, tiled=True)


def from_behind(value, axis):
    count = lax.axis_size(axis)
    return lax.ppermute(value, axis, [(source, source + 1) for source in range(count - 1)])


def swapped(value):
    return lax.ppermute(value, "core", [(0, 1), (1, 0)])


def pair_then_chips(kept, given):
    both = (kept.astype(F32) + swapped(given).astype(F32)).astype(BF16)
    return exchange(both, "x")


def local(
    residual,
    values,
    gate_input,
    group_keys,
    time_step,
    decay_rate,
    skip_gain,
    conv_values,
    conv_keys,
    mix_gain,
    out_weight,
    norm_gain,
    hidden_gate,
    hidden_up,
    hidden_conv,
    hidden_down,
):
    rows, cols = values.shape
    key_cols = group_keys.shape[1]
    last = rows // 8 - 1
    whole = lambda a: pl.BlockSpec(a.shape, lambda i: (0, 0))
    own_rows, tail = call(
        pack_kernel,
        [
            ((hidden_gate.shape[0] * 3 // 2, 2 * hidden_gate.shape[1]), BF16),
            ((8, cols + key_cols), BF16),
        ],
        grid=(1,),
        in_specs=[whole(hidden_gate), whole(hidden_up), whole(hidden_gate)]
        + [pl.BlockSpec((8, width), lambda i: (last, 0)) for width in (cols, key_cols)],
        grant=60,
        name="pack",
    )(hidden_gate, hidden_up, hidden_down.T, values, group_keys)
    weights = lax.all_gather(own_rows, SP, axis=0)
    chips = lax.axis_size("x")
    n_tp = chips * lax.axis_size("core")
    n_row = lax.axis_size(SP[1])
    features = residual.shape[0]
    units = hidden_gate.shape[1]
    before = from_behind(tail, SP)
    core = lax.axis_index("core").astype(jnp.int32).reshape(1)
    span = STATE_WIDE // n_row + STATE_NARROW // n_row + 8
    x, keys, run, delta, run_col, pay = call(
        state_kernel,
        [
            ((rows, cols), BF16),
            ((rows, key_cols), BF16),
            ((GROUP_HEADS, rows), F32),
            ((GROUP_HEADS, rows), F32),
            ((rows, GROUP_HEADS), F32),
            ((n_row, span, HALF), BF16),
        ],
        [((rows + 8, cols), F32), ((rows + 8, key_cols), F32)],
        in_specs=[VMEM, VMEM, VMEM, VMEM, SMEM, VMEM, VMEM],
        grant=60,
        name="span_state",
    )(
        values,
        group_keys,
        before,
        time_step,
        decay_rate,
        conv_values,
        conv_keys,
    )
    by_row = exchange(pay, SP[1])
    base, slope = call(
        inside_kernel, [((rows, cols), F32), ((rows, cols), F32)], name="inside_span"
    )(x, keys, run, delta, run_col, jnp.repeat(skip_gain, HEAD_SIZE).reshape(1, -1), gate_input)
    (sums,) = call(
        row_total_kernel, [((lax.axis_size(SP[0]), span, HALF), BF16)], name="row_total"
    )(by_row)
    totals = exchange(sums, SP[0])
    place = lax.axis_index(SP[0]).astype(jnp.int32).reshape(1)
    (starts,) = call(
        prefix_kernel,
        [((n_row, span - 8, HALF), BF16)],
        in_specs=[
            pl.BlockSpec(memory_space=pltpu.SMEM),
            pl.BlockSpec(memory_space=pltpu.VMEM),
            pl.BlockSpec(memory_space=pltpu.VMEM),
        ],
        name="prefix",
    )(place, by_row, totals)
    carried = exchange(starts, SP[1])
    kept, given = call(
        apply_kernel,
        [((chips, rows + 16, features), BF16)] * 2,
        in_specs=[SMEM] + [VMEM] * 6,
        name="apply_project",
    )(core, base, slope, keys, carried, mix_gain.reshape(1, -1), out_weight)
    summed = pair_then_chips(kept, given)
    place_tp = lax.axis_index(("x", "core"))
    own_gain = lax.dynamic_slice_in_dim(norm_gain, place_tp * features, features, 0)
    lifted, tile, merged = call(
        functools.partial(merge_kernel, cols * n_tp),
        [((rows, features), BF16), ((8, features), BF16), ((features, rows), BF16)],
        name="merge",
    )(summed, residual, own_gain.reshape(1, -1))
    stream = jnp.concatenate([lifted, tile, from_behind(tile, SP)], axis=0)
    own_core = exchange(jnp.broadcast_to(stream, (chips, *stream.shape)), "x")
    other_core = swapped(own_core)
    spans, each = weights.shape[0], hidden_gate.shape[0]
    given, hidden, down = call(
        functools.partial(channel_kernel, features * n_tp),
        [
            ((chips, features, rows), BF16),
            ((rows, units), BF16),
            ((spans, each // 2, 2 * units), BF16),
        ],
        [
            ((rows + 16, features * n_tp), BF16),
            ((spans, each, 2 * units), BF16),
            ((rows + 8, 2 * units), F32),
            ((rows + 16, 2 * units), F32),
        ],
        more_scratch=[pltpu.SemaphoreType.DMA((6,))],
        grant=24,
        in_specs=[SMEM, VMEM, VMEM, pl.BlockSpec(memory_space=pltpu.HBM), VMEM],
        out_specs=[VMEM] * 3,
        name="channel_mixer",
    )(
        core, own_core, other_core, pltpu.with_memory_space_constraint(weights, pltpu.HBM), hidden_conv
    )
    (kept,) = call(
        keep_kernel,
        [((chips, features, rows), BF16)],
        in_specs=[SMEM, VMEM, VMEM],
        out_specs=[VMEM],
        name="keep_blocks",
    )(core, hidden, down)
    got = pair_then_chips(kept, given)
    (out,) = call(finish_kernel, [((features, rows), BF16)], name="finish")(merged, got)
    return out


def solution(mesh):
    split = Mesh(mesh.devices.reshape(8, 8, 4, 2), ("sp_0", "sp_1", "x", "core"))
    tp = ("x", "core")
    placed = (
        P(tp, SP),
        P(SP, tp),
        P(SP, tp),
        P(SP, tp),
        P(tp, SP),
        P(tp),
        P(tp),
        P(None, tp),
        P(None, tp),
        P(tp),
        P(tp, None),
        P(),
        P(SP, tp),
        P(SP, tp),
        P(None, None, tp),
        P(tp, SP),
    )
    return jax.shard_map(local, mesh=split, in_specs=placed, out_specs=P(tp, SP), check_vma=False)
```
